256 devices in a mesh: ep: 64 (over z, x, core), tp: 4 (over y).
Axes of the slice: x: 4, y: 4, z: 8, core: 2. Of those that a mesh axis runs over, the one named last changes fastest.
Arguments:
- head_inputs_unfiltered: bfloat16 [8192, 4096], P('ep', 'tp'), may hold values from -6 to 6
- group_write_vectors: bfloat16 [8192, 512], P('ep', 'tp'), may hold values from -6 to 6
- group_read_vectors: bfloat16 [8192, 512], P('ep', 'tp'), may hold values from -6 to 6
- output_gate_inputs: bfloat16 [8192, 4096], P('ep', 'tp'), may hold values from -6 to 6
- step_preactivation: float32 [64, 8192], P('tp', 'ep'), may hold values from -3.2 to 3.6
- extra_decay_logs: float32 [64, 8192], P('tp', 'ep'), may hold values from -0.7 to 0
- head_decay_logs: float32 [64], P('tp'), may hold values from -16 to -2.7
- head_filter_taps: bfloat16 [4, 4096], P(None, 'tp'), may hold values from -3 to 3
- write_filter_taps: bfloat16 [4, 512], P(None, 'tp'), may hold values from -3 to 3
- read_filter_taps: bfloat16 [4, 512], P(None, 'tp'), may hold values from -3 to 3
- grouped_norm_gain: float32 [4096], P('tp'), may hold values from 0.1 to 1.9
- mixer_output_weight: bfloat16 [4096, 2048], P('tp'), may hold values from -0.09375 to 0.09375
- expert_input_rows: bfloat16 [32768, 2048], P(('ep', 'tp')), may hold values from -6 to 6
- expert_norm_gain: float32 [2048], replicated, may hold values from 0.1 to 1.9
- routes: int32 [32768, 2], P(('ep', 'tp')), may hold values from 0 to 63, all different within a row; in each aligned block of 128 rows (0 to 127, 128 to 255, ...) at most 6 rows name the same one
- router_chosen_scores: bfloat16 [32768, 2], P(('ep', 'tp')), may hold values from 0.049804688 to 1
- routed_gate_weight: bfloat16 [64, 2048, 1024], P('ep', None, 'tp'), may hold values from -0.125 to 0.125
- routed_up_weight: bfloat16 [64, 2048, 1024], P('ep', None, 'tp'), may hold values from -0.125 to 0.125
- routed_down_weight: bfloat16 [64, 1024, 2048], P('ep', 'tp'), may hold values from -0.1875 to 0.1875
- shared_gate_weight: bfloat16 [2048, 512], P(None, 'tp'), may hold values from -0.125 to 0.125
- shared_up_weight: bfloat16 [2048, 512], P(None, 'tp'), may hold values from -0.125 to 0.125
- shared_down_weight: bfloat16 [512, 2048], P('tp'), may hold values from -0.25 to 0.25
Outputs:
- mixer_result: bfloat16 [8192, 2048], P(('ep', 'tp'))
- moe_result: bfloat16 [32768, 2048], P(('ep', 'tp'))
The draws below stay inside these ranges and needn't reach their ends.
Inputs may be any that keep to these rules, and one draw needn't show every extreme that they name: `routes`: within the 128 rows of one device no expert is named more than 6 times; a row names 2 different experts.
All inputs are finite; a program needn't handle non-finite values.
Results may differ from the reference program's by a relative error of at most 0.0095.
Values may be sent and summed in bfloat16 or wider, within the bound.
A program may use at most 128 MiB of HBM per device.

```python
import math
import jax
import jax.numpy as jnp
import numpy as np
from jax import lax

D = 2048
HEADS = 64
HEAD_DIM = 64
GROUPS = 4
STATE = 128
CONV = 4
BLOCK = 64
INNER = 4096
MIX_ROWS = 128
MIX_TOKENS = 8192
EXPERT_FF = 1024
SHARED_FF = 512
EXPERTS = 64
TOP_K = 2
MOE_ROWS = 128
MOE_TOKENS = 32768
CAPACITY = 6
N_TP = 4


def draw_step_preactivation(key, part):
    key_noise, key_shift = jax.random.split(key)
    block_total = MIX_TOKENS // MIX_ROWS
    noise = jnp.clip(0.7 * jax.random.normal(key_noise, (HEADS, MIX_TOKENS), jnp.float32), -1.6, 1.6)
    shifts = jax.random.uniform(key_shift, (block_total,), jnp.float32, -1.0, 1.5)
    return noise + jnp.repeat(shifts, MIX_ROWS)[None, :]


def draw_extra_decay_logs(key, part):
    key_place, key_depth = jax.random.split(key)
    stride = MIX_TOKENS // 3
    places = jnp.arange(3, dtype=jnp.int32) * stride + jax.random.randint(key_place, (3,), 0, stride)
    kept = jax.random.uniform(key_depth, (3, HEADS), jnp.float32, 0.5, 0.8)
    positions = jnp.arange(MIX_TOKENS, dtype=jnp.int32)
    hits = (positions[None, :] == places[:, None]).astype(jnp.float32)
    return jnp.einsum('bh,bt->ht', jnp.log(kept), hits)


def draw_head_decay_logs(key, part):
    key_kind, key_fast, key_slow = jax.random.split(key, 3)
    fast_share = 0.5
    is_fast = jax.random.uniform(key_kind, (HEADS,), jnp.float32) < fast_share
    fast_log = jax.random.uniform(key_fast, (HEADS,), jnp.float32, math.log(1.0 / 40.0), math.log(1.0 / 15.0))
    slow_log = jax.random.uniform(key_slow, (HEADS,), jnp.float32, math.log(0.02), math.log(0.25)) - math.log(float(MIX_TOKENS))
    return jnp.where(is_fast, fast_log, slow_log)


def shard_levels(key, shape, cuts, smallest, high):
    loudness, own = 1.0, jax.random.fold_in(key, 6)
    for position, blocks in cuts:
        draws = jnp.exp(jax.random.uniform(jax.random.fold_in(own, position), (blocks,), jnp.float32, smallest / len(cuts), high / len(cuts)))
        loudness = loudness * jnp.repeat(draws, shape[position] // blocks).reshape([-1 if axis == position else 1 for axis in range(len(shape))])
    return loudness


def deal_out(key, own, number, rows, amount, top, limit, skew):
    sequence = jax.random.permutation(key, amount)
    packed, ordinary = load_shares(amount, rows * top, limit, skew, True), load_shares(amount, rows * top, limit, skew, False)
    places = jnp.arange(amount)

    def named(tallies, rotation):
        used = int((tallies > 0).sum())
        fixed = max(1, used // 4)
        passed = fixed + (places - fixed + rotation * (used - fixed)) % max(1, amount - fixed)
        return jnp.zeros((amount,), jnp.int32).at[sequence[jnp.where(places < fixed, places, passed)]].set(jnp.asarray(tallies, jnp.int32))

    tallies = jnp.where(number % 4 == 0, named(packed, number // 4), named(ordinary, number - number // 4 - 1))
    mixed = jax.random.permutation(jax.random.fold_in(own, 3), amount)
    giver, taker = mixed[0:amount // 2 * 2:2], mixed[1:amount // 2 * 2:2]
    margin = jnp.minimum(tallies[giver] - 1, limit - tallies[taker]) // 2
    margin = jnp.where((giver == sequence[0]) | (taker == sequence[0]) | (tallies[taker] == 0), 0, jnp.maximum(margin, 0))
    passed = jax.random.randint(jax.random.fold_in(own, 4), (amount // 2,), 0, 1 << 20) % (margin + 1)
    tallies = tallies.at[giver].add(-passed).at[taker].add(passed)
    items = jnp.searchsorted(jnp.cumsum(tallies), jnp.arange(rows * top), side="right").astype(jnp.int32)
    grid = items.reshape(top, rows).T
    grid = grid[jax.random.permutation(jax.random.fold_in(own, 1), rows)]
    rotation = jax.random.randint(jax.random.fold_in(own, 2), (rows, 1), 0, top)
    return jnp.take_along_axis(grid, (jnp.arange(top)[None, :] + rotation) % top, axis=1)


def load_shares(number_of, total, most, lean, full):
    weights = [(1 << 20) // math.isqrt(grade ** lean) + 1 for grade in range(1, number_of + 1)]
    largest = most if full else min(most, max(-(-total // number_of), total * weights[0] // sum(weights)))
    least = 1 if total - largest >= number_of - 1 else 0
    counts, surplus = [largest] + [least] * (number_of - 1), total - largest - least * (number_of - 1)
    while surplus > 0:
        candidates = [i for i in range(1, number_of) if counts[i] < largest] or [i for i in range(1, number_of) if counts[i] < most]
        whole, remaining = sum([weights[i] for i in candidates]), surplus
        for i in candidates:
            more = min(most - counts[i], max(1, remaining * weights[i] // whole), surplus)
            counts[i] = counts[i] + more
            surplus = surplus - more
    return np.array(counts)


def scatter_about(key, dims, deviation, bound, pieces=(), kind=jnp.bfloat16):
    level = shard_levels(key, dims, pieces, -0.22, 0.18) if pieces else 1.0
    result = jax.random.normal(key, dims, jnp.float32) * deviation * level
    return jnp.minimum(jnp.maximum(result, -bound), bound).astype(kind)


def setup_inputs(seed: int = 0) -> dict:
    streams_of = jax.random.split(jax.random.key(seed), 23)
    head_inputs_unfiltered = scatter_about(streams_of[0], (MIX_TOKENS, INNER), 1.0, 6.0, ((0, 64), (1, 4)))
    group_write_vectors = scatter_about(streams_of[1], (MIX_TOKENS, GROUPS * STATE), 1.0, 6.0, ((0, 64), (1, 4)))
    group_read_vectors = scatter_about(streams_of[2], (MIX_TOKENS, GROUPS * STATE), 1.0, 6.0, ((0, 64), (1, 4)))
    output_gate_inputs = scatter_about(streams_of[3], (MIX_TOKENS, INNER), 1.0, 6.0, ((0, 64), (1, 4)))
    step_preactivation = draw_step_preactivation(jax.random.fold_in(streams_of[22], 71), 0)
    extra_decay_logs = draw_extra_decay_logs(jax.random.fold_in(streams_of[22], 71), 0)
    head_decay_logs = draw_head_decay_logs(jax.random.fold_in(streams_of[22], 71), 0)
    head_filter_taps = scatter_about(streams_of[7], (CONV, INNER), 0.5, 3.0, ((1, 4),))
    write_filter_taps = scatter_about(streams_of[8], (CONV, GROUPS * STATE), 0.5, 3.0, ((1, 4),))
    read_filter_taps = scatter_about(streams_of[9], (CONV, GROUPS * STATE), 0.5, 3.0, ((1, 4),))
    grouped_norm_gain = jnp.clip(1.0 + 0.18 * jax.random.normal(streams_of[10], (INNER,), jnp.float32), 0.1, 1.9)
    mixer_output_weight = scatter_about(streams_of[11], (INNER, D), INNER ** -0.5, 0.09375, ((0, 4),))
    expert_input_rows = scatter_about(streams_of[12], (MOE_TOKENS, D), 1.0, 6.0, ((0, 256),))
    expert_norm_gain = jnp.clip(1.0 + 0.18 * jax.random.normal(streams_of[13], (D,), jnp.float32), 0.1, 1.9)
    routes_keys = jax.random.split(jax.random.fold_in(streams_of[14], 1), MOE_TOKENS // MOE_ROWS)
    routes_turns = jax.random.permutation(jax.random.fold_in(streams_of[14], 3), MOE_TOKENS // MOE_ROWS)
    routes = jax.vmap(lambda own, number: deal_out(jax.random.fold_in(streams_of[14], 2), own, number, MOE_ROWS, EXPERTS, TOP_K, CAPACITY, 2))(routes_keys, routes_turns).reshape((MOE_TOKENS, TOP_K))
    router_chosen_scores = jnp.clip(jnp.exp(math.log(1.0) - 2.9996462 * jax.random.uniform(streams_of[15], (MOE_TOKENS, TOP_K), jnp.float32) ** shard_levels(streams_of[15], (MOE_TOKENS, TOP_K), ((0, 256),), -0.2, 0.2)), 0.049804688, 1.0).astype(jnp.bfloat16)
    routed_gate_weight = scatter_about(streams_of[16], (EXPERTS, D, EXPERT_FF), D ** -0.5, 0.125, ((0, 64), (2, 4)))
    routed_up_weight = scatter_about(streams_of[17], (EXPERTS, D, EXPERT_FF), D ** -0.5, 0.125, ((0, 64), (2, 4)))
    routed_down_weight = scatter_about(streams_of[18], (EXPERTS, EXPERT_FF, D), EXPERT_FF ** -0.5, 0.1875, ((0, 64), (1, 4)))
    shared_gate_weight = scatter_about(streams_of[19], (D, SHARED_FF), D ** -0.5, 0.125, ((1, 4),))
    shared_up_weight = scatter_about(streams_of[20], (D, SHARED_FF), D ** -0.5, 0.125, ((1, 4),))
    shared_down_weight = scatter_about(streams_of[21], (SHARED_FF, D), SHARED_FF ** -0.5, 0.25, ((0, 4),))
    return dict(head_inputs_unfiltered=head_inputs_unfiltered, group_write_vectors=group_write_vectors, group_read_vectors=group_read_vectors, output_gate_inputs=output_gate_inputs, step_preactivation=step_preactivation, extra_decay_logs=extra_decay_logs, head_decay_logs=head_decay_logs, head_filter_taps=head_filter_taps, write_filter_taps=write_filter_taps, read_filter_taps=read_filter_taps, grouped_norm_gain=grouped_norm_gain, mixer_output_weight=mixer_output_weight, expert_input_rows=expert_input_rows, expert_norm_gain=expert_norm_gain, routes=routes, router_chosen_scores=router_chosen_scores, routed_gate_weight=routed_gate_weight, routed_up_weight=routed_up_weight, routed_down_weight=routed_down_weight, shared_gate_weight=shared_gate_weight, shared_up_weight=shared_up_weight, shared_down_weight=shared_down_weight)


eps_norm = 1e-06
route_scale = 2.5
highest = lax.Precision.HIGHEST

def causal_conv(values, weights):
    taps = weights.shape[0]
    length = values.shape[0]
    padded = jnp.concatenate([jnp.zeros((taps - 1, values.shape[1]), jnp.float32), values.astype(jnp.float32)], axis=0)
    running_sum = jnp.zeros((length, values.shape[1]), jnp.float32)
    for offset in range(taps):
        running_sum = running_sum + weights[offset].astype(jnp.float32) * padded[offset:offset + length]
    return jax.nn.silu(running_sum)

def state_space(head_values, write_values, read_values, step_length_value, decay_rate_logs):
    length = head_values.shape[0]
    block_count = length // BLOCK
    per_group = HEADS // GROUPS
    head_blocks = head_values.reshape(block_count, BLOCK, GROUPS, per_group, HEAD_DIM)
    write_blocks = write_values.reshape(block_count, BLOCK, GROUPS, STATE)
    read_blocks = read_values.reshape(block_count, BLOCK, GROUPS, STATE)
    step_blocks = step_length_value.T.reshape(block_count, BLOCK, GROUPS, per_group)
    rate_blocks = decay_rate_logs.T.reshape(block_count, BLOCK, GROUPS, per_group)
    lower_mask = jnp.tril(jnp.ones((BLOCK, BLOCK), bool))

    def advance(carried, block_data):
        head_blk, write_blk, read_blk, step_blk, rate_blk = block_data
        cumulative = jnp.cumsum(rate_blk, axis=0)
        weighted = head_blk * step_blk[..., None]
        gap_logs = cumulative[:, None] - cumulative[None, :]
        within = jnp.exp(jnp.where(lower_mask[:, :, None, None], gap_logs, -jnp.inf))
        affinity = jnp.einsum('lgn,sgn->lsg', read_blk, write_blk, precision=highest)
        local_part = jnp.einsum('lsge,sgep->lgep', affinity[..., None] * within, weighted, precision=highest)
        carried_part = jnp.einsum('lgn,gepn->lgep', read_blk, carried, precision=highest) * jnp.exp(cumulative)[..., None]
        to_end = jnp.exp(cumulative[-1:] - cumulative)
        new_state = carried * jnp.exp(cumulative[-1])[..., None, None] + jnp.einsum('sgn,sgep->gepn', write_blk, weighted * to_end[..., None], precision=highest)
        return (new_state, local_part + carried_part)
    initial = jnp.zeros((GROUPS, per_group, HEAD_DIM, STATE), jnp.float32)
    _, outputs = lax.scan(advance, initial, (head_blocks, write_blocks, read_blocks, step_blocks, rate_blocks))
    return outputs.reshape(length, HEADS * HEAD_DIM)

def reference(head_inputs_unfiltered, group_write_vectors, group_read_vectors, output_gate_inputs, step_preactivation, extra_decay_logs, head_decay_logs, head_filter_taps, write_filter_taps, read_filter_taps, grouped_norm_gain, mixer_output_weight, expert_input_rows, expert_norm_gain, routes, router_chosen_scores, routed_gate_weight, routed_up_weight, routed_down_weight, shared_gate_weight, shared_up_weight, shared_down_weight):
    length = head_inputs_unfiltered.shape[0]
    head_values = causal_conv(head_inputs_unfiltered, head_filter_taps)
    write_values = causal_conv(group_write_vectors, write_filter_taps)
    read_values = causal_conv(group_read_vectors, read_filter_taps)
    step_length_value = jax.nn.softplus(step_preactivation)
    decay_rate_logs = -jnp.exp(head_decay_logs)[:, None] * step_length_value + extra_decay_logs
    scan_out = state_space(head_values, write_values, read_values, step_length_value, decay_rate_logs)
    gated = scan_out * jax.nn.silu(output_gate_inputs.astype(jnp.float32))
    grouped = gated.reshape(length, GROUPS, HEADS * HEAD_DIM // GROUPS)
    grouped = grouped * lax.rsqrt(lax.optimization_barrier(jnp.mean(grouped * grouped, axis=-1, keepdims=True)) + eps_norm)
    mixer_normed = (grouped.reshape(length, HEADS * HEAD_DIM) * grouped_norm_gain).astype(jnp.bfloat16)
    mixer_result = jnp.dot(mixer_normed, mixer_output_weight, preferred_element_type=jnp.float32).astype(jnp.bfloat16)
    rows_float = expert_input_rows.astype(jnp.float32)
    moe_normed = (rows_float * lax.rsqrt(lax.optimization_barrier(jnp.mean(rows_float * rows_float, axis=-1, keepdims=True)) + eps_norm) * expert_norm_gain).astype(jnp.bfloat16)
    score_float = router_chosen_scores.astype(jnp.float32)
    route_weight = score_float / lax.optimization_barrier(jnp.sum(score_float, axis=-1, keepdims=True)) * route_scale
    token_total = expert_input_rows.shape[0]
    device_total = token_total // MOE_ROWS
    flat_expert = routes.reshape(device_total, MOE_ROWS * TOP_K)
    onehot = (flat_expert[:, :, None] == jnp.arange(EXPERTS, dtype=jnp.int32)[None, None, :]).astype(jnp.int32)
    before = jnp.cumsum(onehot, axis=1) - onehot
    slot_rank = lax.optimization_barrier(jnp.sum(before * onehot, axis=2))
    slot_index = jnp.arange(device_total, dtype=jnp.int32)[:, None] * CAPACITY + slot_rank
    token_index = jnp.arange(token_total * TOP_K, dtype=jnp.int32) // TOP_K
    table_token = jnp.full((EXPERTS, device_total * CAPACITY), token_total, jnp.int32).at[flat_expert.reshape(-1), slot_index.reshape(-1)].set(token_index)
    table_weight = jnp.zeros((EXPERTS, device_total * CAPACITY), jnp.float32).at[flat_expert.reshape(-1), slot_index.reshape(-1)].set(route_weight.reshape(-1))
    padded_rows = jnp.concatenate([moe_normed, jnp.zeros((1, D), jnp.bfloat16)], axis=0)
    slice_width = EXPERT_FF // N_TP

    def one_expert(running_sum, expert_data):
        tokens_here, weights_here, gate_weight, up_weight, down_weight = expert_data
        picked = padded_rows[tokens_here]
        gate_value = jnp.dot(picked, gate_weight, preferred_element_type=jnp.float32)
        up_value = jnp.dot(picked, up_weight, preferred_element_type=jnp.float32)
        hidden = (jax.nn.silu(gate_value) * up_value).astype(jnp.bfloat16)
        summed = jnp.zeros((picked.shape[0], D), jnp.float32)
        for slice_index in range(N_TP):
            lower_edge = slice_index * slice_width
            part = jnp.dot(hidden[:, lower_edge:lower_edge + slice_width], down_weight[lower_edge:lower_edge + slice_width], preferred_element_type=jnp.float32).astype(jnp.bfloat16)
            summed = summed + part.astype(jnp.float32)
        return (running_sum.at[tokens_here].add(summed * weights_here[:, None]), None)
    routed, _ = lax.scan(one_expert, jnp.zeros((token_total + 1, D), jnp.float32), (table_token, table_weight, routed_gate_weight, routed_up_weight, routed_down_weight))
    shared_hidden = (jax.nn.silu(jnp.dot(moe_normed, shared_gate_weight, preferred_element_type=jnp.float32)) * jnp.dot(moe_normed, shared_up_weight, preferred_element_type=jnp.float32)).astype(jnp.bfloat16)
    shared_total = jnp.dot(shared_hidden, shared_down_weight, preferred_element_type=jnp.float32)
    moe_result = (shared_total + routed[:token_total]).astype(jnp.bfloat16)
    return (mixer_result, moe_result)
```

```python
import jax
import jax.numpy as jnp
import numpy as np
from jax import lax
from jax.experimental import pallas as pl
from jax.experimental.pallas import tpu as pltpu
from jax.sharding import Mesh
from jax.sharding import PartitionSpec as P

HEAD_DIM = 64
STATE = 128
CAP = 6
SIZES = (128, 256, 256, 256, 256, 256, 256, 256, 128)
CHUNKS = len(SIZES)
COLS = tuple(slice(sum(SIZES[:c]), sum(SIZES[: c + 1])) for c in range(CHUNKS))
Z, X, G, Y = 8, 4, 8, 4
EP = ("ep_0", "ep_1", "ep_2")
EP_TP = ("ep_0", "ep_1", "ep_2", "tp")
MESH = pl.DeviceIdType.MESH

eps_norm = 1e-06
route_scale = 2.5
highest = lax.Precision.HIGHEST
f32 = jnp.float32
bf16 = jnp.bfloat16


class Names:
    def __init__(self, names, refs):
        self.__dict__.update(zip(names, refs))


def dot(a, b, precision=None):
    return jnp.dot(a, b, preferred_element_type=f32, precision=precision)


def dot_t(a, b, precision=None):
    return lax.dot_general(
        a, b, (((0,), (0,)), ((), ())), preferred_element_type=f32, precision=precision
    )


def silu(v):
    return v * (1.0 / (1.0 + jnp.exp(-v)))


def make_kernel(inputs, scratch):
    def kernel(*refs):
        n = len(inputs)
        body(Names(inputs, refs[:n]), refs[n], refs[n + 1], Names(scratch, refs[n + 2 :]))

    return kernel


def body(i, mix_out, moe_out, s):
    z = lax.axis_index("ep_0")
    x = lax.axis_index("ep_1")
    core = lax.axis_index("ep_2")
    y = lax.axis_index("tp")
    g = x * 2 + core
    ep = z * G + g
    width = i.rows.shape[1]
    ff = i.gate_w.shape[2]
    tok = i.rows.shape[0]
    slots = Z * G * CAP
    zrows = G * CAP
    n_pos = i.heads.shape[0]
    chans = i.heads.shape[1]
    heads = i.step.shape[0]
    per = chans // G

    def z_peer(d):
        return (lax.rem(z + d, Z), x, core, y)

    def g_peer(d):
        t = lax.rem(g + d, G)
        return (z, lax.div(t, 2), lax.rem(t, 2), y)

    def x_peer(d):
        return (z, lax.rem(x + d, X), core, y)

    def y_peer(d):
        return (z, x, core, lax.rem(y + d, Y))

    def ep_peer(d):
        t = lax.rem(ep + d + Z * G, Z * G)
        r = lax.rem(t, G)
        return (lax.div(t, G), lax.div(r, 2), lax.rem(r, 2), y)

    pair_y = y + 1 - 2 * lax.rem(y, 2)
    weight_pair = (z, x, core, pair_y)
    token_pair = (z, x, core, Y - 1 - y)
    sibling = (z, x, 1 - core, y)

    def rc(src, dst, send, recv, dev):
        return pltpu.make_async_remote_copy(
            src_ref=src, dst_ref=dst, send_sem=send, recv_sem=recv, device_id=dev, device_id_type=MESH
        )

    def drain(ref, sem):
        pltpu.make_async_copy(ref, ref, sem).wait()

    barrier = pltpu.get_barrier_semaphore()

    def greet(dev):
        pl.semaphore_signal(barrier, inc=1, device_id=dev, device_id_type=MESH)

    @pl.loop(1, Z)
    def _(d):
        greet(z_peer(d))
        greet(g_peer(d))

    @pl.loop(1, Y)
    def _(d):
        greet(y_peer(d))

    greet(ep_peer(1))
    greet(ep_peer(-1))

    def tail_copies():
        last = pl.ds(n_pos - 16, 16)
        dev = ep_peer(1)
        return [
            rc(src.at[last, :], dst, s.tail_s.at[k], s.tail_r.at[k], dev)
            for k, (src, dst) in enumerate(
                ((i.heads, s.tail_heads), (i.write, s.tail_write), (i.read, s.tail_read))
            )
        ]

    def weight_copy(k, c):
        src = (i.gate_w, i.up_w, i.down_w)[k].at[0]
        if k < 2:
            src, dst = src.at[COLS[c], :], s.pgu.at[k, COLS[c], :]
        else:
            src, dst = src.at[:, COLS[c]], s.pdown.at[:, COLS[c]]
        return rc(src, dst, s.w_s.at[k // 2], s.w_r.at[k // 2, c], weight_pair)

    shared_full = (s.full_gate, s.full_up, s.full_down)

    def piece(t, slot, q, count=1):
        ref = shared_full[t]
        n = ref.shape[1] // G
        return ref.at[slot, pl.ds(pl.multiple_of(q * n, n), count * n), :]

    def sh_y(t):
        q = core * X + x
        return rc(piece(t, 0, q), piece(t, 1, q), s.shy_s.at[t], s.shy_r.at[t], token_pair)

    def sh_x_start(t, d):
        part = piece(t, 1, core * X + x)
        rc(part, part, s.shx_s.at[t], s.shx_r.at[t], x_peer(d)).start()

    def sh_x_drain(t, sem):
        drain(piece(t, 1, 0, X - 1), sem.at[t])

    def sh_c(t):
        part = piece(t, 1, core * X, X)
        return rc(part, part, s.shc_s.at[t], s.shc_r.at[t], sibling)

    def shared_rows():
        return rc(s.normed, s.pair_normed, s.st_s.at[0], s.st_r.at[0], weight_pair)

    def shared_return():
        return rc(s.sh_send, s.sh_recv, s.st_s.at[1], s.st_r.at[1], weight_pair)

    def sy(c):
        part = (slice(None), slice(None), COLS[c])
        return rc(s.toks.at[0].at[part], s.toks.at[1].at[part], s.y_s.at[0], s.y_r.at[0, c], token_pair)

    def ry(c):
        return rc(s.ysend.at[:, COLS[c]], s.yrecv.at[:, COLS[c]], s.y_s.at[1], s.y_r.at[1, c], token_pair)

    def spread_z(src, dst, c, k):
        @pl.loop(1, Z)
        def _(d):
            rc(
                src.at[lax.rem(z + d, Z), :, COLS[c]], dst.at[z, :, COLS[c]], s.z_s.at[k], s.z_r.at[k, c], z_peer(d)
            ).start()

    def spread_g(src, dst, c, k):
        @pl.loop(1, G)
        def _(d):
            rc(
                src.at[lax.rem(g + d, G), :, COLS[c]], dst.at[g, :, COLS[c]], s.g_s.at[k], s.g_r.at[k, c], g_peer(d)
            ).start()

    def seven(ref, c, sem, k):
        drain(ref.at[pl.ds(0, 7), :, COLS[c]], sem.at[k, c])

    def mix_g(src, dst, k, d):
        rc(src.at[lax.rem(g + d, G)], dst.at[g], s.m_s.at[k], s.m_r.at[k], g_peer(d)).start()

    def mix_drain(ref, sem, k):
        drain(ref.at[pl.ds(0, 7)], sem.at[k])

    bring = []

    def fetched(src, dst):
        bring.append((src, dst))
        return pltpu.make_async_copy(src, dst, s.loc.at[len(bring) - 1])

    small_in = [
        fetched(src, dst)
        for src, dst in (
            (i.routes, s.routes),
            (i.scores, s.scores),
            (i.row_gain, s.row_gain),
            (i.rows, s.rows),
            (i.write, s.write),
            (i.read, s.read),
            (i.step, s.step),
            (i.extra, s.extra),
            (i.decay, s.decay),
            (i.head_taps, s.head_taps),
            (i.write_taps, s.write_taps),
            (i.read_taps, s.read_taps),
            (i.mix_gain, s.mix_gain),
        )
    ]
    local = dict(
        heads=fetched(i.heads, s.heads),
        gates=fetched(i.gates, s.gates),
        perm=fetched(i.perm, s.perm),
        sh_gate=fetched(i.sh_gate, s.full_gate.at[0]),
        sh_up=fetched(i.sh_up, s.full_up.at[0]),
        sh_down=fetched(i.sh_down, s.full_down.at[0]),
        gate=fetched(i.gate_w.at[0], s.ogate),
        up=fetched(i.up_w.at[0], s.oup),
        down=fetched(i.down_w.at[0], s.odown),
        mixw=fetched(i.mix_weight, s.mixw),
    )
    for copy in small_in + list(local.values()):
        copy.start()
    local = Names(local.keys(), local.values())
    for copy in small_in[:4]:
        copy.wait()
    route = s.routes[...]
    score = s.scores[...].astype(f32)
    weight = score / jnp.sum(score, axis=0, keepdims=True) * route_scale
    expert_iota = lax.broadcasted_iota(jnp.int32, (Z * G, tok), 0)
    hot = [(route[k : k + 1, :] == expert_iota).astype(f32) for k in range(2)]
    earlier = (
        lax.broadcasted_iota(jnp.int32, (tok, tok), 0) < lax.broadcasted_iota(jnp.int32, (tok, tok), 1)
    ).astype(bf16)
    before = dot((hot[0] + hot[1]).astype(bf16), earlier)
    slot_iota = lax.broadcasted_iota(jnp.int32, (slots, tok), 0)
    pick = jnp.zeros((slots, tok), f32)
    pick_w = jnp.zeros((slots, tok), f32)
    for k in range(2):
        rank = jnp.sum(before * hot[k], axis=0, keepdims=True).astype(jnp.int32)
        here = slot_iota == route[k : k + 1, :] * CAP + rank
        pick = pick + here.astype(f32)
        pick_w = pick_w + jnp.where(here, weight[k : k + 1, :], 0.0)
    s.pick_w[...] = pick_w
    pick = pick.astype(bf16)
    rows = s.rows[...].astype(f32)
    normed = (
        rows * lax.rsqrt(jnp.mean(rows * rows, axis=1, keepdims=True) + eps_norm) * s.row_gain[...]
    ).astype(bf16)
    s.normed[...] = normed
    pl.semaphore_wait(barrier, (Z - 1) + (G - 1) + (Y - 1) + 2)

    def select(c):
        part = dot(pick, s.normed[:, COLS[c]]).astype(bf16)
        s.own[:, :, COLS[c]] = part.reshape(Z, zrows, -1)
        spread_z(s.own, s.recv1, c, 0)

    weight_copy(0, 0).start()
    weight_copy(1, 0).start()
    select(0)
    for copy in tail_copies():
        copy.start()
    for t in range(3):
        (local.sh_gate, local.sh_up, local.sh_down)[t].wait()
        sh_y(t).start()
    for c in range(1, CHUNKS):
        weight_copy(0, c).start()
        weight_copy(1, c).start()
        select(c)
    for c in range(CHUNKS):
        weight_copy(2, c).start()
    shared_rows().start()
    s.recv1[z] = s.own[z]

    ext = s.ext

    def mixer_conv():
        local.heads.wait()
        for copy in tail_copies():
            copy.wait_recv()
        has_before = (ep > 0).astype(f32)
        for copy in small_in[4:]:
            copy.wait()
        col = 0
        for src, tail in ((s.heads, s.tail_heads), (s.write, s.tail_write), (s.read, s.tail_read)):
            w = src.shape[1]
            ext[0:16, col : col + w] = tail[...].astype(f32) * has_before
            ext[16 : 16 + n_pos, col : col + w] = src[...].astype(f32)
            col += w

        def conv(taps_ref, col):
            w = taps_ref.shape[1]
            taps = taps_ref[...].astype(f32)
            total = jnp.zeros((n_pos, w), f32)
            for j in range(taps.shape[0]):
                total = total + taps[j : j + 1, :] * ext[13 + j : 13 + j + n_pos, col : col + w]
            return silu(total)

        s.hv[...] = conv(s.head_taps, 0)
        s.wv[...] = conv(s.write_taps, chans)
        s.rv[...] = conv(s.read_taps, chans + STATE)

    def row_col():
        return (
            lax.broadcasted_iota(jnp.int32, (n_pos, n_pos), 0),
            lax.broadcasted_iota(jnp.int32, (n_pos, n_pos), 1),
        )

    def mixer_states():
        pre = s.step[...]
        step = jnp.maximum(pre, 0.0) + jnp.log1p(jnp.exp(-jnp.abs(pre)))
        eye = lax.broadcasted_iota(jnp.int32, (heads, heads), 0) == lax.broadcasted_iota(
            jnp.int32, (heads, heads), 1
        )
        decay = jnp.sum(jnp.where(eye, s.decay[...], 0.0), axis=1, keepdims=True)
        rate = -jnp.exp(decay) * step + s.extra[...]
        pos_r, pos_c = row_col()
        cum = dot(rate, (pos_r <= pos_c).astype(f32), highest)
        s.cum[...] = cum
        total_decay = cum[:, n_pos - 1 : n_pos]
        lane = lax.broadcasted_iota(jnp.int32, (heads, chans), 1)
        first = lax.broadcasted_iota(jnp.int32, (heads, chans), 0) * HEAD_DIM
        spread = ((lane >= first) & (lane < first + HEAD_DIM)).astype(f32)
        xw = s.hv[...] * dot_t(step, spread, highest)
        s.hv[...] = xw
        s.cum_x[...] = dot_t(jnp.exp(cum), spread, highest)
        xe = xw * dot_t(jnp.exp(total_decay - cum), spread, highest)
        decay_x = dot_t(jnp.broadcast_to(total_decay, (heads, 8)), spread, highest)
        states = dot_t(s.wv[...], xe, highest)
        for j in range(G):
            s.st_send[j] = states[:, j * per : (j + 1) * per].astype(bf16)
            s.dec_send[j] = decay_x[:, j * per : (j + 1) * per]
        s.st_got[g] = s.st_send[g]
        s.dec_got[g] = s.dec_send[g]
        s.affinity[...] = lax.dot_general(
            s.rv[...], s.wv[...], (((1,), (1,)), ((), ())), preferred_element_type=f32, precision=highest
        )

    def mixer_scan(pairs):
        cum = s.cum[...]
        cum_t = jnp.transpose(cum)
        affinity = s.affinity[...]
        pos_r, pos_c = row_col()
        low = pos_r >= pos_c
        pair_lane = lax.broadcasted_iota(jnp.int32, (n_pos, 2 * HEAD_DIM), 1) < HEAD_DIM
        for p in pairs:
            cols = slice(p * 2 * HEAD_DIM, (p + 1) * 2 * HEAD_DIM)
            xp = s.hv[:, cols]
            both = []
            for h in (2 * p, 2 * p + 1):
                gap = cum_t[:, h : h + 1] - cum[h : h + 1, :]
                within = jnp.exp(jnp.where(low, gap, -jnp.inf))
                both.append(dot(affinity * within, xp, highest))
            s.scan[:, cols] = jnp.where(pair_lane, both[0], both[1])

    def mixer_group():
        mix_drain(s.st_got, s.m_r, 0)
        mix_drain(s.dec_got, s.m_r, 3)
        run = jnp.zeros((STATE, per), f32)
        run_d = jnp.zeros((8, per), f32)
        for j in range(G):
            s.enter[j, 0:STATE, :] = run
            s.enter[j, STATE : STATE + 8, :] = run_d
            d_j = s.dec_got[j]
            run = s.st_got[j].astype(f32) + jnp.exp(d_j[0:1, :]) * run
            run_d = run_d + d_j
        s.tot_send[0:STATE, :] = run
        s.tot_send[STATE : STATE + 8, :] = run_d

        @pl.loop(1, Z)
        def _(d):
            rc(s.tot_send, s.tot_got.at[z], s.m_s.at[1], s.m_r.at[1], z_peer(d)).start()

        s.tot_got[z] = s.tot_send[...]

    def mixer_enter():
        mix_drain(s.tot_got, s.m_r, 1)
        run = jnp.zeros((STATE, per), f32)
        for j in range(Z):
            new = s.tot_got[j, 0:STATE, :] + jnp.exp(s.tot_got[j, STATE : STATE + 1, :]) * run
            run = jnp.where(j < z, new, run)
        for j in range(G):
            entry = s.enter[j, 0:STATE, :] + jnp.exp(s.enter[j, STATE : STATE + 1, :]) * run
            s.in_send[j] = entry.astype(bf16)
        for d in range(1, G):
            mix_g(s.in_send, s.in_got, 2, d)
        s.in_got[g] = s.in_send[g]

    def mixer_finish():
        mix_drain(s.in_got, s.m_r, 2)
        local.gates.wait()
        rv = s.rv[...]
        square = jnp.zeros((n_pos, 1), f32)
        for j in range(G):
            cols = slice(j * per, (j + 1) * per)
            carried = dot(rv, s.in_got[j].astype(f32), highest) * s.cum_x[:, cols]
            gated = (s.scan[:, cols] + carried) * silu(s.gates[:, cols].astype(f32))
            s.scan[:, cols] = gated
            square = square + jnp.sum(gated * gated, axis=1, keepdims=True)
        scale = lax.rsqrt(square / chans + eps_norm)
        mixed = (s.scan[...] * scale * s.mix_gain[...]).astype(bf16)
        local.mixw.wait()
        mb = n_pos // Y
        for c in range(4):
            cols = slice(c * (width // 4), (c + 1) * (width // 4))
            part = dot(mixed, s.mixw[:, cols]).astype(bf16)
            for j in range(Y):
                s.mix_send[j, :, cols] = part[j * mb : (j + 1) * mb, :]
        s.mix_got[y] = s.mix_send[y]

    def mixer_send():
        @pl.loop(1, Y)
        def _(d):
            rc(
                s.mix_send.at[lax.rem(y + d, Y)], s.mix_got.at[y], s.rs_s.at[0], s.rs_r.at[0], y_peer(d)
            ).start()

    def shared_x(t, d):
        if d == 1:
            sh_y(t).wait_recv()
        sh_x_start(t, d)

    def shared_c():
        for t in range(3):
            sh_x_drain(t, s.shx_r)
            sh_c(t).start()

    def shared_hidden(v, slot):
        return (silu(dot(v, s.full_gate[slot])) * dot(v, s.full_up[slot])).astype(bf16)

    def shared_down(h, q):
        cols = slice(q * (width // 4), (q + 1) * (width // 4))
        return cols, dot(h[0], s.full_down[0, :, cols]) + dot(h[1], s.full_down[1, :, cols])

    def shared_own():
        for t in range(3):
            sh_c(t).wait_recv()
        v = s.normed[...]
        h = (shared_hidden(v, 0), shared_hidden(v, 1))
        for q in range(4):
            cols, new = shared_down(h, q)
            s.sh_own[:, cols] = new

    def shared_pair():
        shared_rows().wait_recv()
        v = s.pair_normed[...]
        h = (shared_hidden(v, 0), shared_hidden(v, 1))
        for q in range(4):
            cols, new = shared_down(h, q)
            s.sh_send[:, cols] = new.astype(bf16)
        shared_return().start()

    def stage_a(c):
        seven(s.recv1, c, s.z_r, 0)
        moved = dot(s.perm[...], s.recv1[:, :, COLS[c]].reshape(slots, -1)).astype(bf16)
        s.perm1[:, :, COLS[c]] = moved.reshape(G, Z * CAP, -1)
        spread_g(s.perm1, s.toks.at[0], c, 0)
        s.toks[0, g, :, COLS[c]] = s.perm1[g, :, COLS[c]]

    def gate_up(t, c):
        v = s.toks[t, :, :, COLS[c]].reshape(slots, -1)
        for acc, refs in ((s.accg, (s.ogate, s.pgu.at[0])), (s.accu, (s.oup, s.pgu.at[1]))):
            for n, ref in enumerate(refs):
                cols = slice(n * ff, (n + 1) * ff)
                new = dot(v, ref[COLS[c], :])
                if c > 0:
                    new = new + acc[t, :, cols]
                acc[t, :, cols] = new

    def stage_b(c):
        seven(s.toks.at[0], c, s.g_r, 0)
        sy(c).start()

    def own_rows(c):
        if c == 0:
            local.gate.wait()
            local.up.wait()
        drain(s.pgu.at[:, COLS[c], :], s.w_r.at[0, c])
        gate_up(0, c)

    def pair_rows(c):
        sy(c).wait_recv()
        gate_up(1, c)

    def hide(t):
        s.hidden[t] = (silu(s.accg[t]) * s.accu[t]).astype(bf16)

    def down(t, c):
        return dot(s.hidden[t, :, 0:ff], s.odown[:, COLS[c]]) + dot(s.hidden[t, :, ff : 2 * ff], s.pdown[:, COLS[c]])

    def back_d(c):
        if c >= CHUNKS:
            return
        if c == 0:
            local.down.wait()
        weight_copy(2, c).wait_recv()
        s.ysend[:, COLS[c]] = down(1, c).astype(bf16)
        ry(c).start()

    def back_e(c):
        mine = down(0, c)
        ry(c).wait_recv()
        total = (mine + s.yrecv[:, COLS[c]].astype(f32)).astype(bf16)
        s.back2[:, :, COLS[c]] = total.reshape(G, Z * CAP, -1)
        spread_g(s.back2, s.got2, c, 1)
        s.got2[g, :, COLS[c]] = s.back2[g, :, COLS[c]]

    def back_f(c):
        seven(s.got2, c, s.g_r, 1)
        moved = dot(s.perm[...], s.got2[:, :, COLS[c]].reshape(slots, -1)).astype(bf16)
        s.back1[:, :, COLS[c]] = moved.reshape(Z, zrows, -1)
        spread_z(s.back1, s.got1, c, 1)
        s.got1[z, :, COLS[c]] = s.back1[z, :, COLS[c]]

    def weights_by_row():
        pick_w = jnp.transpose(s.pick_w[...])
        w_hi = pick_w.astype(bf16)
        s.w_hi[...] = w_hi
        s.w_lo[...] = (pick_w - w_hi.astype(f32)).astype(bf16)

    def early_sends():
        for copy in tail_copies():
            copy.wait_send()
        drain(s.pgu, s.w_s.at[0])
        drain(s.pdown, s.w_s.at[1])
        drain(s.toks.at[0], s.y_s.at[0])
        drain(s.own.at[pl.ds(0, Z - 1)], s.z_s.at[0])
        drain(s.perm1.at[pl.ds(0, G - 1)], s.g_s.at[0])
        for t in range(3):
            sh_y(t).wait_send()
            sh_x_drain(t, s.shx_s)
            sh_c(t).wait_send()
        mix_drain(s.st_got, s.m_s, 0)
        mix_drain(s.dec_got, s.m_s, 3)
        mix_drain(s.tot_got, s.m_s, 1)
        mix_drain(s.in_got, s.m_s, 2)

    extras = {
        1: lambda: mixer_states(),
        2: lambda: mixer_scan(range(0, 2)),
        3: lambda: mixer_scan(range(2, 4)),
        4: lambda: mixer_scan(range(4, 6)),
        5: lambda: mixer_scan(range(6, 8)),
    }
    spare = [(t, d) for t in range(3) for d in range(1, X)]
    mixer_conv()
    local.perm.wait()
    for c in range(CHUNKS):
        stage_a(c)
        if c >= 1:
            stage_b(c - 1)
        if c in extras:
            extras[c]()
        if 1 <= c < G:
            mix_g(s.st_send, s.st_got, 0, c)
            mix_g(s.dec_send, s.dec_got, 3, c)
        if c >= 2:
            for t, d in spare[2 * (c - 2) : 2 * (c - 1)]:
                shared_x(t, d)
            own_rows(c - 2)
        if c >= 4:
            pair_rows(c - 4)
    stage_b(CHUNKS - 1)
    mixer_group()
    shared_c()
    for c in range(CHUNKS - 4, CHUNKS):
        if c >= CHUNKS - 2:
            own_rows(c)
        pair_rows(c)
    hide(1)
    back_d(0)
    back_d(1)
    hide(0)
    back_d(2)
    after = {
        0: lambda: mixer_enter(),
        2: lambda: mixer_finish(),
        3: lambda: shared_own(),
        4: lambda: weights_by_row(),
        5: lambda: shared_pair(),
        7: lambda: early_sends(),
        CHUNKS: lambda: mixer_send(),
    }
    for c in range(CHUNKS + 1):
        back_d(c + 3)
        if c < CHUNKS:
            back_e(c)
        if c >= 1:
            back_f(c - 1)
        if c in after:
            after[c]()

    def moe_copy(c):
        return pltpu.make_async_copy(s.moe_res.at[:, COLS[c]], moe_out.at[:, COLS[c]], s.out.at[0])

    def mix_sum():
        drain(s.mix_got.at[pl.ds(0, Y - 1)], s.rs_r.at[0])
        mix = jnp.zeros(s.mix_res.shape, f32)
        for j in range(Y):
            mix = mix + s.mix_got[j].astype(f32)
        s.mix_res[...] = mix.astype(bf16)

    mix_copy = pltpu.make_async_copy(s.mix_res, mix_out, s.out.at[1])
    shared_rows().wait_send()
    shared_return().wait()
    drain(s.ysend, s.y_s.at[1])
    for c in range(CHUNKS):
        if c == CHUNKS - 1:
            drain(s.back2.at[pl.ds(0, G - 1)], s.g_s.at[1])
            drain(s.back1.at[pl.ds(0, Z - 1)], s.z_s.at[1])
            mix_sum()
            mix_copy.start()
            drain(s.mix_send.at[pl.ds(0, Y - 1)], s.rs_s.at[0])
        seven(s.got1, c, s.z_r, 1)
        v = s.got1[:, :, COLS[c]].reshape(slots, -1)
        shared = s.sh_own[:, COLS[c]] + s.sh_recv[:, COLS[c]].astype(f32)
        total = dot(s.w_hi[...], v) + dot(s.w_lo[...], v) + shared
        s.moe_res[:, COLS[c]] = total.astype(bf16)
        moe_copy(c).start()
    mix_copy.wait()
    drain(s.moe_res, s.out.at[0])


def local(
    heads, write, read, gates, step, extra, decay, head_taps, write_taps, read_taps, mix_gain,
    mix_weight, rows, row_gain, routes, scores, gate_w, up_w, down_w, sh_gate, sh_up, sh_down,
):
    n_pos, chans = heads.shape
    tok, width = rows.shape
    ff = gate_w.shape[2]
    sff = sh_gate.shape[1]
    slots = Z * G * CAP
    per = chans // G
    order = np.arange(slots).reshape(G, Z, CAP).transpose(1, 0, 2).reshape(-1)
    perm = jnp.asarray(np.eye(slots, dtype=np.float32)[order], bf16)
    dma = pltpu.SemaphoreType.DMA
    blocks = (Z, G * CAP, width)
    scratch = dict(
        tail_heads=((16, chans), bf16),
        tail_write=((16, STATE), bf16),
        tail_read=((16, STATE), bf16),
        ogate=((width, ff), bf16),
        oup=((width, ff), bf16),
        odown=((ff, width), bf16),
        pgu=((2, width, ff), bf16),
        pdown=((ff, width), bf16),
        mixw=((chans, width), bf16),
        full_gate=((2, width, sff), bf16),
        full_up=((2, width, sff), bf16),
        full_down=((2, sff, width), bf16),
        pair_normed=((tok, width), bf16),
        sh_send=((tok, width), bf16),
        sh_recv=((tok, width), bf16),
        gates=((n_pos, chans), bf16),
        normed=((tok, width), bf16),
        sh_own=((tok, width), f32),
        pick_w=((slots, tok), f32),
        w_hi=((tok, slots), bf16),
        w_lo=((tok, slots), bf16),
        own=(blocks, bf16),
        recv1=(blocks, bf16),
        perm1=(blocks, bf16),
        toks=((2, *blocks), bf16),
        accg=((2, slots, 2 * ff), f32),
        accu=((2, slots, 2 * ff), f32),
        hidden=((2, slots, 2 * ff), bf16),
        ysend=((slots, width), bf16),
        yrecv=((slots, width), bf16),
        back2=(blocks, bf16),
        got2=(blocks, bf16),
        back1=(blocks, bf16),
        got1=(blocks, bf16),
        ext=((n_pos + 16, chans + 2 * STATE), f32),
        hv=((n_pos, chans), f32),
        wv=((n_pos, STATE), f32),
        rv=((n_pos, STATE), f32),
        cum=((step.shape[0], n_pos), f32),
        affinity=((n_pos, n_pos), f32),
        cum_x=((n_pos, chans), f32),
        scan=((n_pos, chans), f32),
        st_send=((G, STATE, per), bf16),
        st_got=((G, STATE, per), bf16),
        dec_send=((G, 8, per), f32),
        dec_got=((G, 8, per), f32),
        enter=((G, STATE + 8, per), f32),
        tot_send=((STATE + 8, per), f32),
        tot_got=((Z, STATE + 8, per), f32),
        in_send=((G, STATE, per), bf16),
        in_got=((G, STATE, per), bf16),
        mix_send=((Y, n_pos // Y, width), bf16),
        mix_got=((Y, n_pos // Y, width), bf16),
        mix_res=((n_pos // Y, width), bf16),
        moe_res=((tok, width), bf16),
    )
    sems = dict(
        tail_s=(3,), tail_r=(3,), w_s=(2,), w_r=(2, CHUNKS), shy_s=(3,), shy_r=(3,), shx_s=(3,), shx_r=(3,), shc_s=(3,),
        shc_r=(3,), st_s=(2,), st_r=(2,), z_s=(2,), z_r=(2, CHUNKS), g_s=(2,), g_r=(2, CHUNKS), y_s=(2,),
        y_r=(2, CHUNKS), m_s=(4,), m_r=(4,), rs_s=(1,), rs_r=(1,), loc=(23,), out=(2,),
    )
    inputs = dict(
        gates=gates, mix_weight=mix_weight, gate_w=gate_w, up_w=up_w, down_w=down_w, sh_gate=sh_gate, sh_up=sh_up,
        sh_down=sh_down,
    )
    copied = dict(
        heads=heads, write=write, read=read, step=step, extra=extra, decay=decay.reshape(1, -1), head_taps=head_taps,
        write_taps=write_taps, read_taps=read_taps, mix_gain=mix_gain.reshape(1, -1), rows=rows,
        row_gain=row_gain.reshape(1, -1), routes=routes.T, scores=scores.T, perm=perm,
    )
    scratch.update((n, (v.shape, v.dtype)) for n, v in copied.items())
    inputs.update(copied)
    names = list(scratch) + list(sems)
    shapes = [pltpu.VMEM(*v) for v in scratch.values()] + [dma(v) for v in sems.values()]
    hbm = pl.BlockSpec(memory_space=pl.ANY)
    return pl.pallas_call(
        make_kernel(list(inputs), names),
        name="mixer_moe",
        out_shape=(
            jax.ShapeDtypeStruct((n_pos // Y, width), bf16),
            jax.ShapeDtypeStruct((tok, width), bf16),
        ),
        in_specs=[hbm] * len(inputs),
        out_specs=(hbm, hbm),
        scratch_shapes=shapes,
        compiler_params=pltpu.CompilerParams(
            collective_id=0, has_side_effects=True, vmem_limit_bytes=67043328
        ),
    )(*inputs.values())


def solution(mesh):
    split = Mesh(mesh.devices.reshape(8, 4, 2, mesh.shape["tp"]), ("ep_0", "ep_1", "ep_2", "tp"))
    placed = (
        P(EP, "tp"),
        P(EP, "tp"),
        P(EP, "tp"),
        P(EP, "tp"),
        P("tp", EP),
        P("tp", EP),
        P("tp"),
        P(None, "tp"),
        P(None, "tp"),
        P(None, "tp"),
        P("tp"),
        P("tp", None),
        P(EP_TP, None),
        P(),
        P(EP_TP, None),
        P(EP_TP, None),
        P(EP, None, "tp"),
        P(EP, None, "tp"),
        P(EP, "tp", None),
        P(None, "tp"),
        P(None, "tp"),
        P("tp", None),
    )
    return jax.shard_map(
        local,
        mesh=split,
        in_specs=placed,
        out_specs=(P(EP_TP, None), P(EP_TP, None)),
        check_vma=False,
    )
```

```python
import jax
import jax.numpy as jnp
import numpy as np
from jax import lax
from jax.experimental import pallas as pl
from jax.experimental.pallas import tpu as pltpu
from jax.sharding import Mesh
from jax.sharding import PartitionSpec as P

HEAD_DIM = 64
STATE = 128
CAP = 6
SIZES = (128, 256, 256, 256, 256, 256, 256, 128, 128, 128)
CHUNKS = len(SIZES)
COLS = tuple(slice(sum(SIZES[:c]), sum(SIZES[: c + 1])) for c in range(CHUNKS))
Z, X, G, Y = 8, 4, 8, 4
EP = ("ep_0", "ep_1", "ep_2")
EP_TP = ("ep_0", "ep_1", "ep_2", "tp")
MESH = pl.DeviceIdType.MESH

eps_norm = 1e-06
route_scale = 2.5
highest = lax.Precision.HIGHEST
f32 = jnp.float32
bf16 = jnp.bfloat16


class Names:
    def __init__(self, names, refs):
        self.__dict__.update(zip(names, refs))


def dot(a, b, precision=None):
    return jnp.dot(a, b, preferred_element_type=f32, precision=precision)


def dot_t(a, b, precision=None):
    return lax.dot_general(
        a, b, (((0,), (0,)), ((), ())), preferred_element_type=f32, precision=precision
    )


def silu(v):
    return v * (1.0 / (1.0 + jnp.exp(-v)))


def make_kernel(inputs, scratch):
    def kernel(*refs):
        n = len(inputs)
        body(Names(inputs, refs[:n]), refs[n], refs[n + 1], Names(scratch, refs[n + 2 :]))

    return kernel


def body(i, mix_out, moe_out, s):
    z = lax.axis_index("ep_0")
    x = lax.axis_index("ep_1")
    core = lax.axis_index("ep_2")
    y = lax.axis_index("tp")
    g = x * 2 + core
    ep = z * G + g
    width = i.rows.shape[1]
    ff = i.gate_w.shape[2]
    tok = i.rows.shape[0]
    slots = Z * G * CAP
    zrows = G * CAP
    n_pos = i.heads.shape[0]
    chans = i.heads.shape[1]
    heads = i.step.shape[0]
    per = chans // G

    def z_peer(d):
        return (lax.rem(z + d, Z), x, core, y)

    def g_peer(d):
        t = lax.rem(g + d, G)
        return (z, lax.div(t, 2), lax.rem(t, 2), y)

    def x_peer(d):
        return (z, lax.rem(x + d, X), core, y)

    def y_peer(d):
        return (z, x, core, lax.rem(y + d, Y))

    def ep_peer(d):
        t = lax.rem(ep + d + Z * G, Z * G)
        r = lax.rem(t, G)
        return (lax.div(t, G), lax.div(r, 2), lax.rem(r, 2), y)

    pair_y = y + 1 - 2 * lax.rem(y, 2)
    weight_pair = (z, x, core, pair_y)
    token_pair = (z, x, core, Y - 1 - y)
    sibling = (z, x, 1 - core, y)

    def rc(src, dst, send, recv, dev):
        return pltpu.make_async_remote_copy(
            src_ref=src, dst_ref=dst, send_sem=send, recv_sem=recv, device_id=dev, device_id_type=MESH
        )

    def drain(ref, sem):
        pltpu.make_async_copy(ref, ref, sem).wait()

    barrier = pltpu.get_barrier_semaphore()

    def greet(dev):
        pl.semaphore_signal(barrier, inc=1, device_id=dev, device_id_type=MESH)

    @pl.loop(1, Z)
    def _(d):
        greet(z_peer(d))
        greet(g_peer(d))

    @pl.loop(1, Y)
    def _(d):
        greet(y_peer(d))

    greet(ep_peer(1))
    greet(ep_peer(-1))

    def tail_copies():
        last = pl.ds(n_pos - 16, 16)
        dev = ep_peer(1)
        return [
            rc(src.at[last, :], dst, s.tail_s.at[k], s.tail_r.at[k], dev)
            for k, (src, dst) in enumerate(
                ((i.heads, s.tail_heads), (i.write, s.tail_write), (i.read, s.tail_read))
            )
        ]

    def weight_copy(k, c):
        src = (i.gate_w, i.up_w, i.down_w)[k].at[0]
        if k < 2:
            src, dst = src.at[COLS[c], :], s.pgu.at[k, COLS[c], :]
        else:
            src, dst = src.at[:, COLS[c]], s.pdown.at[:, COLS[c]]
        return rc(src, dst, s.w_s.at[k // 2], s.w_r.at[k // 2, c], weight_pair)

    shared_full = (s.full_gate, s.full_up, s.full_down)

    def piece(t, slot, q, count=1):
        ref = shared_full[t]
        n = ref.shape[1] // G
        return ref.at[slot, pl.ds(pl.multiple_of(q * n, n), count * n), :]

    def sh_y(t):
        q = core * X + x
        return rc(piece(t, 0, q), piece(t, 1, q), s.shy_s.at[t], s.shy_r.at[t], token_pair)

    def sh_x_start(t, d):
        part = piece(t, 1, core * X + x)
        rc(part, part, s.shx_s.at[t], s.shx_r.at[t], x_peer(d)).start()

    def sh_x_drain(t, sem):
        drain(piece(t, 1, 0, X - 1), sem.at[t])

    def sh_c(t):
        part = piece(t, 1, core * X, X)
        return rc(part, part, s.shc_s.at[t], s.shc_r.at[t], sibling)

    def shared_rows():
        return rc(s.normed, s.pair_normed, s.st_s.at[0], s.st_r.at[0], weight_pair)

    def shared_return():
        return rc(s.sh_send, s.sh_recv, s.st_s.at[1], s.st_r.at[1], weight_pair)

    def sy(c):
        part = (slice(None), slice(None), COLS[c])
        return rc(s.toks.at[0].at[part], s.toks.at[1].at[part], s.y_s.at[0], s.y_r.at[0, c], token_pair)

    def ry(c):
        return rc(s.ysend.at[:, COLS[c]], s.yrecv.at[:, COLS[c]], s.y_s.at[1], s.y_r.at[1, c], token_pair)

    def spread_z(src, dst, c, k):
        @pl.loop(1, Z)
        def _(d):
            rc(
                src.at[lax.rem(z + d, Z), :, COLS[c]], dst.at[z, :, COLS[c]], s.z_s.at[k], s.z_r.at[k, c], z_peer(d)
            ).start()

    def spread_g(src, dst, c, k):
        @pl.loop(1, G)
        def _(d):
            rc(
                src.at[lax.rem(g + d, G), :, COLS[c]], dst.at[g, :, COLS[c]], s.g_s.at[k], s.g_r.at[k, c], g_peer(d)
            ).start()

    def seven(ref, c, sem, k):
        drain(ref.at[pl.ds(0, 7), :, COLS[c]], sem.at[k, c])

    def mix_g(src, dst, k, d):
        rc(src.at[lax.rem(g + d, G)], dst.at[g], s.m_s.at[k], s.m_r.at[k], g_peer(d)).start()

    def mix_drain(ref, sem, k):
        drain(ref.at[pl.ds(0, 7)], sem.at[k])

    bring = []

    def fetched(src, dst):
        bring.append((src, dst))
        return pltpu.make_async_copy(src, dst, s.loc.at[len(bring) - 1])

    small_in = [
        fetched(src, dst)
        for src, dst in (
            (i.routes, s.routes),
            (i.scores, s.scores),
            (i.row_gain, s.row_gain),
            (i.rows, s.rows),
            (i.write, s.write),
            (i.read, s.read),
            (i.step, s.step),
            (i.extra, s.extra),
            (i.decay, s.decay),
            (i.head_taps, s.head_taps),
            (i.write_taps, s.write_taps),
            (i.read_taps, s.read_taps),
            (i.mix_gain, s.mix_gain),
        )
    ]
    local = dict(
        heads=fetched(i.heads, s.heads),
        gates=fetched(i.gates, s.gates),
        perm=fetched(i.perm, s.perm),
        sh_gate=fetched(i.sh_gate, s.full_gate.at[0]),
        sh_up=fetched(i.sh_up, s.full_up.at[0]),
        sh_down=fetched(i.sh_down, s.full_down.at[0]),
        gate=fetched(i.gate_w.at[0], s.ogate),
        up=fetched(i.up_w.at[0], s.oup),
        down=fetched(i.down_w.at[0], s.odown),
        mixw=fetched(i.mix_weight, s.mixw),
    )
    for copy in small_in + list(local.values()):
        copy.start()
    local = Names(local.keys(), local.values())
    for copy in small_in[:4]:
        copy.wait()
    route = s.routes[...]
    score = s.scores[...].astype(f32)
    weight = score / jnp.sum(score, axis=0, keepdims=True) * route_scale
    expert_iota = lax.broadcasted_iota(jnp.int32, (Z * G, tok), 0)
    hot = [(route[k : k + 1, :] == expert_iota).astype(f32) for k in range(2)]
    earlier = (
        lax.broadcasted_iota(jnp.int32, (tok, tok), 0) < lax.broadcasted_iota(jnp.int32, (tok, tok), 1)
    ).astype(bf16)
    before = dot((hot[0] + hot[1]).astype(bf16), earlier)
    slot_iota = lax.broadcasted_iota(jnp.int32, (slots, tok), 0)
    pick = jnp.zeros((slots, tok), f32)
    pick_w = jnp.zeros((slots, tok), f32)
    for k in range(2):
        rank = jnp.sum(before * hot[k], axis=0, keepdims=True).astype(jnp.int32)
        here = slot_iota == route[k : k + 1, :] * CAP + rank
        pick = pick + here.astype(f32)
        pick_w = pick_w + jnp.where(here, weight[k : k + 1, :], 0.0)
    s.pick_w[...] = pick_w
    pick = pick.astype(bf16)
    rows = s.rows[...].astype(f32)
    normed = (
        rows * lax.rsqrt(jnp.mean(rows * rows, axis=1, keepdims=True) + eps_norm) * s.row_gain[...]
    ).astype(bf16)
    s.normed[...] = normed
    pl.semaphore_wait(barrier, (Z - 1) + (G - 1) + (Y - 1) + 2)

    def select(c):
        part = dot(pick, s.normed[:, COLS[c]]).astype(bf16)
        s.own[:, :, COLS[c]] = part.reshape(Z, zrows, -1)
        spread_z(s.own, s.recv1, c, 0)

    weight_copy(0, 0).start()
    weight_copy(1, 0).start()
    select(0)
    for copy in tail_copies():
        copy.start()
    for t in range(3):
        (local.sh_gate, local.sh_up, local.sh_down)[t].wait()
        sh_y(t).start()
    for c in range(1, CHUNKS):
        weight_copy(0, c).start()
        weight_copy(1, c).start()
        select(c)
    for c in range(CHUNKS):
        weight_copy(2, c).start()
    shared_rows().start()
    s.recv1[z] = s.own[z]

    ext = s.ext

    def mixer_conv():
        local.heads.wait()
        for copy in tail_copies():
            copy.wait_recv()
        has_before = (ep > 0).astype(f32)
        for copy in small_in[4:]:
            copy.wait()
        col = 0
        for src, tail in ((s.heads, s.tail_heads), (s.write, s.tail_write), (s.read, s.tail_read)):
            w = src.shape[1]
            ext[0:16, col : col + w] = tail[...].astype(f32) * has_before
            ext[16 : 16 + n_pos, col : col + w] = src[...].astype(f32)
            col += w

        def conv(taps_ref, col):
            w = taps_ref.shape[1]
            taps = taps_ref[...].astype(f32)
            total = jnp.zeros((n_pos, w), f32)
            for j in range(taps.shape[0]):
                total = total + taps[j : j + 1, :] * ext[13 + j : 13 + j + n_pos, col : col + w]
            return silu(total)

        s.hv[...] = conv(s.head_taps, 0)
        s.wv[...] = conv(s.write_taps, chans)
        s.rv[...] = conv(s.read_taps, chans + STATE)

    def row_col():
        return (
            lax.broadcasted_iota(jnp.int32, (n_pos, n_pos), 0),
            lax.broadcasted_iota(jnp.int32, (n_pos, n_pos), 1),
        )

    def mixer_states():
        pre = s.step[...]
        step = jnp.maximum(pre, 0.0) + jnp.log1p(jnp.exp(-jnp.abs(pre)))
        eye = lax.broadcasted_iota(jnp.int32, (heads, heads), 0) == lax.broadcasted_iota(
            jnp.int32, (heads, heads), 1
        )
        decay = jnp.sum(jnp.where(eye, s.decay[...], 0.0), axis=1, keepdims=True)
        rate = -jnp.exp(decay) * step + s.extra[...]
        pos_r, pos_c = row_col()
        cum = dot(rate, (pos_r <= pos_c).astype(f32), highest)
        s.cum[...] = cum
        total_decay = cum[:, n_pos - 1 : n_pos]
        lane = lax.broadcasted_iota(jnp.int32, (heads, chans), 1)
        first = lax.broadcasted_iota(jnp.int32, (heads, chans), 0) * HEAD_DIM
        spread = ((lane >= first) & (lane < first + HEAD_DIM)).astype(f32)
        xw = s.hv[...] * dot_t(step, spread, highest)
        s.hv[...] = xw
        s.cum_x[...] = dot_t(jnp.exp(cum), spread, highest)
        xe = xw * dot_t(jnp.exp(total_decay - cum), spread, highest)
        decay_x = dot_t(jnp.broadcast_to(total_decay, (heads, 8)), spread, highest)
        states = dot_t(s.wv[...], xe, highest)
        for j in range(G):
            s.st_send[j] = states[:, j * per : (j + 1) * per].astype(bf16)
            s.dec_send[j] = decay_x[:, j * per : (j + 1) * per]
        s.st_got[g] = s.st_send[g]
        s.dec_got[g] = s.dec_send[g]
        s.affinity[...] = lax.dot_general(
            s.rv[...], s.wv[...], (((1,), (1,)), ((), ())), preferred_element_type=f32, precision=highest
        )

    def mixer_scan(pairs):
        cum = s.cum[...]
        cum_t = jnp.transpose(cum)
        affinity = s.affinity[...]
        pos_r, pos_c = row_col()
        low = pos_r >= pos_c
        pair_lane = lax.broadcasted_iota(jnp.int32, (n_pos, 2 * HEAD_DIM), 1) < HEAD_DIM
        for p in pairs:
            cols = slice(p * 2 * HEAD_DIM, (p + 1) * 2 * HEAD_DIM)
            xp = s.hv[:, cols]
            both = []
            for h in (2 * p, 2 * p + 1):
                gap = cum_t[:, h : h + 1] - cum[h : h + 1, :]
                within = jnp.exp(jnp.where(low, gap, -jnp.inf))
                both.append(dot(affinity * within, xp, highest))
            s.scan[:, cols] = jnp.where(pair_lane, both[0], both[1])

    def mixer_group():
        mix_drain(s.st_got, s.m_r, 0)
        mix_drain(s.dec_got, s.m_r, 3)
        run = jnp.zeros((STATE, per), f32)
        run_d = jnp.zeros((8, per), f32)
        for j in range(G):
            s.enter[j, 0:STATE, :] = run
            s.enter[j, STATE : STATE + 8, :] = run_d
            d_j = s.dec_got[j]
            run = s.st_got[j].astype(f32) + jnp.exp(d_j[0:1, :]) * run
            run_d = run_d + d_j
        s.tot_send[0:STATE, :] = run
        s.tot_send[STATE : STATE + 8, :] = run_d

        @pl.loop(1, Z)
        def _(d):
            rc(s.tot_send, s.tot_got.at[z], s.m_s.at[1], s.m_r.at[1], z_peer(d)).start()

        s.tot_got[z] = s.tot_send[...]

    def mixer_enter():
        mix_drain(s.tot_got, s.m_r, 1)
        run = jnp.zeros((STATE, per), f32)
        for j in range(Z):
            new = s.tot_got[j, 0:STATE, :] + jnp.exp(s.tot_got[j, STATE : STATE + 1, :]) * run
            run = jnp.where(j < z, new, run)
        for j in range(G):
            entry = s.enter[j, 0:STATE, :] + jnp.exp(s.enter[j, STATE : STATE + 1, :]) * run
            s.in_send[j] = entry.astype(bf16)
        for d in range(1, G):
            mix_g(s.in_send, s.in_got, 2, d)
        s.in_got[g] = s.in_send[g]

    def mixer_finish():
        mix_drain(s.in_got, s.m_r, 2)
        local.gates.wait()
        rv = s.rv[...]
        square = jnp.zeros((n_pos, 1), f32)
        for j in range(G):
            cols = slice(j * per, (j + 1) * per)
            carried = dot(rv, s.in_got[j].astype(f32), highest) * s.cum_x[:, cols]
            gated = (s.scan[:, cols] + carried) * silu(s.gates[:, cols].astype(f32))
            s.scan[:, cols] = gated
            square = square + jnp.sum(gated * gated, axis=1, keepdims=True)
        scale = lax.rsqrt(square / chans + eps_norm)
        mixed = (s.scan[...] * scale * s.mix_gain[...]).astype(bf16)
        local.mixw.wait()
        mb = n_pos // Y
        for c in range(4):
            cols = slice(c * (width // 4), (c + 1) * (width // 4))
            part = dot(mixed, s.mixw[:, cols]).astype(bf16)
            for j in range(Y):
                s.mix_send[j, :, cols] = part[j * mb : (j + 1) * mb, :]
        s.mix_got[y] = s.mix_send[y]

    def mixer_send():
        @pl.loop(1, Y)
        def _(d):
            rc(
                s.mix_send.at[lax.rem(y + d, Y)], s.mix_got.at[y], s.rs_s.at[0], s.rs_r.at[0], y_peer(d)
            ).start()

    def shared_x(t, d):
        if d == 1:
            sh_y(t).wait_recv()
        sh_x_start(t, d)

    def shared_c():
        for t in range(3):
            sh_x_drain(t, s.shx_r)
            sh_c(t).start()

    def shared_hidden(v, slot):
        return (silu(dot(v, s.full_gate[slot])) * dot(v, s.full_up[slot])).astype(bf16)

    def shared_down(h, q):
        cols = slice(q * (width // 4), (q + 1) * (width // 4))
        return cols, dot(h[0], s.full_down[0, :, cols]) + dot(h[1], s.full_down[1, :, cols])

    def shared_own():
        for t in range(3):
            sh_c(t).wait_recv()
        v = s.normed[...]
        h = (shared_hidden(v, 0), shared_hidden(v, 1))
        for q in range(4):
            cols, new = shared_down(h, q)
            s.sh_own[:, cols] = new

    def shared_pair():
        shared_rows().wait_recv()
        v = s.pair_normed[...]
        h = (shared_hidden(v, 0), shared_hidden(v, 1))
        for q in range(4):
            cols, new = shared_down(h, q)
            s.sh_send[:, cols] = new.astype(bf16)
        shared_return().start()

    def stage_a(c):
        seven(s.recv1, c, s.z_r, 0)
        moved = dot(s.perm[...], s.recv1[:, :, COLS[c]].reshape(slots, -1)).astype(bf16)
        s.perm1[:, :, COLS[c]] = moved.reshape(G, Z * CAP, -1)
        spread_g(s.perm1, s.toks.at[0], c, 0)
        s.toks[0, g, :, COLS[c]] = s.perm1[g, :, COLS[c]]

    def gate_up(t, c):
        v = s.toks[t, :, :, COLS[c]].reshape(slots, -1)
        for acc, refs in ((s.accg, (s.ogate, s.pgu.at[0])), (s.accu, (s.oup, s.pgu.at[1]))):
            for n, ref in enumerate(refs):
                cols = slice(n * ff, (n + 1) * ff)
                new = dot(v, ref[COLS[c], :])
                if c > 0:
                    new = new + acc[t, :, cols]
                acc[t, :, cols] = new

    def stage_b(c):
        seven(s.toks.at[0], c, s.g_r, 0)
        sy(c).start()

    def own_rows(c):
        if c == 0:
            local.gate.wait()
            local.up.wait()
        drain(s.pgu.at[:, COLS[c], :], s.w_r.at[0, c])
        gate_up(0, c)

    def pair_rows(c):
        sy(c).wait_recv()
        gate_up(1, c)

    def hide(t):
        s.hidden[t] = (silu(s.accg[t]) * s.accu[t]).astype(bf16)

    def down(t, c):
        return dot(s.hidden[t, :, 0:ff], s.odown[:, COLS[c]]) + dot(s.hidden[t, :, ff : 2 * ff], s.pdown[:, COLS[c]])

    def back_d(c):
        if c >= CHUNKS:
            return
        if c == 0:
            local.down.wait()
        weight_copy(2, c).wait_recv()
        s.ysend[:, COLS[c]] = down(1, c).astype(bf16)
        ry(c).start()

    def back_e(c):
        mine = down(0, c)
        ry(c).wait_recv()
        total = (mine + s.yrecv[:, COLS[c]].astype(f32)).astype(bf16)
        s.back2[:, :, COLS[c]] = total.reshape(G, Z * CAP, -1)
        spread_g(s.back2, s.got2, c, 1)
        s.got2[g, :, COLS[c]] = s.back2[g, :, COLS[c]]

    def back_f(c):
        seven(s.got2, c, s.g_r, 1)
        moved = dot(s.perm[...], s.got2[:, :, COLS[c]].reshape(slots, -1)).astype(bf16)
        s.back1[:, :, COLS[c]] = moved.reshape(Z, zrows, -1)
        spread_z(s.back1, s.got1, c, 1)
        s.got1[z, :, COLS[c]] = s.back1[z, :, COLS[c]]

    def weights_by_row():
        pick_w = jnp.transpose(s.pick_w[...])
        w_hi = pick_w.astype(bf16)
        s.w_hi[...] = w_hi
        s.w_lo[...] = (pick_w - w_hi.astype(f32)).astype(bf16)

    def early_sends():
        for copy in tail_copies():
            copy.wait_send()
        drain(s.pgu, s.w_s.at[0])
        drain(s.pdown, s.w_s.at[1])
        drain(s.toks.at[0], s.y_s.at[0])
        drain(s.own.at[pl.ds(0, Z - 1)], s.z_s.at[0])
        drain(s.perm1.at[pl.ds(0, G - 1)], s.g_s.at[0])
        for t in range(3):
            sh_y(t).wait_send()
            sh_x_drain(t, s.shx_s)
            sh_c(t).wait_send()
        mix_drain(s.st_got, s.m_s, 0)
        mix_drain(s.dec_got, s.m_s, 3)
        mix_drain(s.tot_got, s.m_s, 1)
        mix_drain(s.in_got, s.m_s, 2)

    extras = {
        1: lambda: mixer_states(),
        2: lambda: mixer_scan(range(0, 2)),
        3: lambda: mixer_scan(range(2, 4)),
        4: lambda: mixer_scan(range(4, 6)),
        5: lambda: mixer_scan(range(6, 8)),
    }
    mixer_conv()
    local.perm.wait()
    for c in range(CHUNKS):
        stage_a(c)
        if c >= 1:
            stage_b(c - 1)
        if c in extras:
            extras[c]()
        if 1 <= c < G:
            mix_g(s.st_send, s.st_got, 0, c)
            mix_g(s.dec_send, s.dec_got, 3, c)
        if c >= 2:
            own_rows(c - 2)
        if c >= 4:
            pair_rows(c - 4)
    stage_b(CHUNKS - 1)
    mixer_group()
    for t in range(3):
        for d in range(1, X):
            shared_x(t, d)
    for c in range(CHUNKS - 4, CHUNKS):
        if c >= CHUNKS - 2:
            own_rows(c)
        pair_rows(c)
    hide(1)
    back_d(0)
    back_d(1)
    hide(0)
    back_d(2)
    after = {
        0: lambda: mixer_enter(),
        1: lambda: shared_c(),
        2: lambda: mixer_finish(),
        3: lambda: shared_own(),
        4: lambda: weights_by_row(),
        5: lambda: shared_pair(),
        7: lambda: early_sends(),
        CHUNKS: lambda: mixer_send(),
    }
    for c in range(CHUNKS + 1):
        back_d(c + 3)
        if c < CHUNKS:
            back_e(c)
        if c >= 1:
            back_f(c - 1)
        if c in after:
            after[c]()

    def moe_copy(c):
        return pltpu.make_async_copy(s.moe_res.at[:, COLS[c]], moe_out.at[:, COLS[c]], s.out.at[0])

    def mix_sum():
        drain(s.mix_got.at[pl.ds(0, Y - 1)], s.rs_r.at[0])
        mix = jnp.zeros(s.mix_res.shape, f32)
        for j in range(Y):
            mix = mix + s.mix_got[j].astype(f32)
        s.mix_res[...] = mix.astype(bf16)

    mix_copy = pltpu.make_async_copy(s.mix_res, mix_out, s.out.at[1])
    shared_rows().wait_send()
    shared_return().wait()
    drain(s.ysend, s.y_s.at[1])
    for c in range(CHUNKS):
        if c == CHUNKS - 1:
            drain(s.back2.at[pl.ds(0, G - 1)], s.g_s.at[1])
            drain(s.back1.at[pl.ds(0, Z - 1)], s.z_s.at[1])
            mix_sum()
            mix_copy.start()
            drain(s.mix_send.at[pl.ds(0, Y - 1)], s.rs_s.at[0])
        seven(s.got1, c, s.z_r, 1)
        v = s.got1[:, :, COLS[c]].reshape(slots, -1)
        shared = s.sh_own[:, COLS[c]] + s.sh_recv[:, COLS[c]].astype(f32)
        total = dot(s.w_hi[...], v) + dot(s.w_lo[...], v) + shared
        s.moe_res[:, COLS[c]] = total.astype(bf16)
        moe_copy(c).start()
    mix_copy.wait()
    drain(s.moe_res, s.out.at[0])


def settle(mix_in, moe_in, mix_out, moe_out, mix, moe, sems):
    pairs = ((mix_in, mix, mix_out), (moe_in, moe, moe_out))
    into = [pltpu.make_async_copy(a, v, sems.at[k]) for k, (a, v, _) in enumerate(pairs)]
    out = [pltpu.make_async_copy(v, b, sems.at[k + 2]) for k, (_, v, b) in enumerate(pairs)]
    for copy in into:
        copy.start()
    for arrived, copy in zip(into, out):
        arrived.wait()
        copy.start()
    for copy in out:
        copy.wait()


def local(
    heads, write, read, gates, step, extra, decay, head_taps, write_taps, read_taps, mix_gain,
    mix_weight, rows, row_gain, routes, scores, gate_w, up_w, down_w, sh_gate, sh_up, sh_down,
):
    n_pos, chans = heads.shape
    tok, width = rows.shape
    ff = gate_w.shape[2]
    sff = sh_gate.shape[1]
    slots = Z * G * CAP
    per = chans // G
    order = np.arange(slots).reshape(G, Z, CAP).transpose(1, 0, 2).reshape(-1)
    perm = jnp.asarray(np.eye(slots, dtype=np.float32)[order], bf16)
    dma = pltpu.SemaphoreType.DMA
    blocks = (Z, G * CAP, width)
    scratch = dict(
        tail_heads=((16, chans), bf16),
        tail_write=((16, STATE), bf16),
        tail_read=((16, STATE), bf16),
        ogate=((width, ff), bf16),
        oup=((width, ff), bf16),
        odown=((ff, width), bf16),
        pgu=((2, width, ff), bf16),
        pdown=((ff, width), bf16),
        mixw=((chans, width), bf16),
        full_gate=((2, width, sff), bf16),
        full_up=((2, width, sff), bf16),
        full_down=((2, sff, width), bf16),
        pair_normed=((tok, width), bf16),
        sh_send=((tok, width), bf16),
        sh_recv=((tok, width), bf16),
        gates=((n_pos, chans), bf16),
        normed=((tok, width), bf16),
        sh_own=((tok, width), f32),
        pick_w=((slots, tok), f32),
        w_hi=((tok, slots), bf16),
        w_lo=((tok, slots), bf16),
        own=(blocks, bf16),
        recv1=(blocks, bf16),
        perm1=(blocks, bf16),
        toks=((2, *blocks), bf16),
        accg=((2, slots, 2 * ff), f32),
        accu=((2, slots, 2 * ff), f32),
        hidden=((2, slots, 2 * ff), bf16),
        ysend=((slots, width), bf16),
        yrecv=((slots, width), bf16),
        back2=(blocks, bf16),
        got2=(blocks, bf16),
        back1=(blocks, bf16),
        got1=(blocks, bf16),
        ext=((n_pos + 16, chans + 2 * STATE), f32),
        hv=((n_pos, chans), f32),
        wv=((n_pos, STATE), f32),
        rv=((n_pos, STATE), f32),
        cum=((step.shape[0], n_pos), f32),
        affinity=((n_pos, n_pos), f32),
        cum_x=((n_pos, chans), f32),
        scan=((n_pos, chans), f32),
        st_send=((G, STATE, per), bf16),
        st_got=((G, STATE, per), bf16),
        dec_send=((G, 8, per), f32),
        dec_got=((G, 8, per), f32),
        enter=((G, STATE + 8, per), f32),
        tot_send=((STATE + 8, per), f32),
        tot_got=((Z, STATE + 8, per), f32),
        in_send=((G, STATE, per), bf16),
        in_got=((G, STATE, per), bf16),
        mix_send=((Y, n_pos // Y, width), bf16),
        mix_got=((Y, n_pos // Y, width), bf16),
        mix_res=((n_pos // Y, width), bf16),
        moe_res=((tok, width), bf16),
    )
    sems = dict(
        tail_s=(3,), tail_r=(3,), w_s=(2,), w_r=(2, CHUNKS), shy_s=(3,), shy_r=(3,), shx_s=(3,), shx_r=(3,), shc_s=(3,),
        shc_r=(3,), st_s=(2,), st_r=(2,), z_s=(2,), z_r=(2, CHUNKS), g_s=(2,), g_r=(2, CHUNKS), y_s=(2,),
        y_r=(2, CHUNKS), m_s=(4,), m_r=(4,), rs_s=(1,), rs_r=(1,), loc=(23,), out=(2,),
    )
    inputs = dict(
        gates=gates, mix_weight=mix_weight, gate_w=gate_w, up_w=up_w, down_w=down_w, sh_gate=sh_gate, sh_up=sh_up,
        sh_down=sh_down,
    )
    copied = dict(
        heads=heads, write=write, read=read, step=step, extra=extra, decay=decay.reshape(1, -1), head_taps=head_taps,
        write_taps=write_taps, read_taps=read_taps, mix_gain=mix_gain.reshape(1, -1), rows=rows,
        row_gain=row_gain.reshape(1, -1), routes=routes.T, scores=scores.T, perm=perm,
    )
    scratch.update((n, (v.shape, v.dtype)) for n, v in copied.items())
    inputs.update(copied)
    names = list(scratch) + list(sems)
    shapes = [pltpu.VMEM(*v) for v in scratch.values()] + [dma(v) for v in sems.values()]
    hbm = pl.BlockSpec(memory_space=pl.ANY)
    outs = (
        jax.ShapeDtypeStruct((n_pos // Y, width), bf16),
        jax.ShapeDtypeStruct((tok, width), bf16),
    )
    results = pl.pallas_call(
        make_kernel(list(inputs), names),
        name="mixer_moe",
        out_shape=outs,
        in_specs=[hbm] * len(inputs),
        out_specs=(hbm, hbm),
        scratch_shapes=shapes,
        compiler_params=pltpu.CompilerParams(
            collective_id=0, has_side_effects=True, vmem_limit_bytes=67043328
        ),
    )(*inputs.values())
    return pl.pallas_call(
        settle,
        name="settle",
        out_shape=outs,
        in_specs=[hbm] * 2,
        out_specs=(hbm, hbm),
        scratch_shapes=[pltpu.VMEM(v.shape, v.dtype) for v in outs] + [dma((4,))],
    )(*results)


def solution(mesh):
    split = Mesh(mesh.devices.reshape(8, 4, 2, mesh.shape["tp"]), ("ep_0", "ep_1", "ep_2", "tp"))
    placed = (
        P(EP, "tp"),
        P(EP, "tp"),
        P(EP, "tp"),
        P(EP, "tp"),
        P("tp", EP),
        P("tp", EP),
        P("tp"),
        P(None, "tp"),
        P(None, "tp"),
        P(None, "tp"),
        P("tp"),
        P("tp", None),
        P(EP_TP, None),
        P(),
        P(EP_TP, None),
        P(EP_TP, None),
        P(EP, None, "tp"),
        P(EP, None, "tp"),
        P(EP, "tp", None),
        P(None, "tp"),
        P(None, "tp"),
        P("tp", None),
    )
    return jax.shard_map(
        local,
        mesh=split,
        in_specs=placed,
        out_specs=(P(EP_TP, None), P(EP_TP, None)),
        check_vma=False,
    )
```

```python
import jax
import jax.numpy as jnp
import numpy as np
from jax import lax
from jax.experimental import pallas as pl
from jax.experimental.pallas import tpu as pltpu
from jax.sharding import Mesh
from jax.sharding import PartitionSpec as P

HEAD_DIM = 64
STATE = 128
CAP = 6
SIZES = (128, 256, 256, 256, 256, 256, 256, 256, 128)
CHUNKS = len(SIZES)
COLS = tuple(slice(sum(SIZES[:c]), sum(SIZES[: c + 1])) for c in range(CHUNKS))
Z, X, G, Y = 8, 4, 8, 4
EP = ("ep_0", "ep_1", "ep_2")
EP_TP = ("ep_0", "ep_1", "ep_2", "tp")
MESH = pl.DeviceIdType.MESH

eps_norm = 1e-06
route_scale = 2.5
highest = lax.Precision.HIGHEST
f32 = jnp.float32
bf16 = jnp.bfloat16


class Names:
    def __init__(self, names, refs):
        self.__dict__.update(zip(names, refs))


def dot(a, b, precision=None):
    return jnp.dot(a, b, preferred_element_type=f32, precision=precision)


def dot_t(a, b, precision=None):
    return lax.dot_general(
        a, b, (((0,), (0,)), ((), ())), preferred_element_type=f32, precision=precision
    )


def silu(v):
    return v * (1.0 / (1.0 + jnp.exp(-v)))


def make_kernel(inputs, scratch):
    def kernel(*refs):
        n = len(inputs)
        body(Names(inputs, refs[:n]), refs[n], refs[n + 1], Names(scratch, refs[n + 2 :]))

    return kernel


def body(i, mix_out, moe_out, s):
    z = lax.axis_index("ep_0")
    x = lax.axis_index("ep_1")
    core = lax.axis_index("ep_2")
    y = lax.axis_index("tp")
    g = x * 2 + core
    ep = z * G + g
    width = i.rows.shape[1]
    ff = i.gate_w.shape[2]
    tok = i.rows.shape[0]
    slots = Z * G * CAP
    zrows = G * CAP
    n_pos = i.heads.shape[0]
    chans = i.heads.shape[1]
    heads = i.step.shape[0]
    per = chans // G

    def z_peer(d):
        return (lax.rem(z + d, Z), x, core, y)

    def g_peer(d):
        t = lax.rem(g + d, G)
        return (z, lax.div(t, 2), lax.rem(t, 2), y)

    def x_peer(d):
        return (z, lax.rem(x + d, X), core, y)

    def y_peer(d):
        return (z, x, core, lax.rem(y + d, Y))

    def ep_peer(d):
        t = lax.rem(ep + d + Z * G, Z * G)
        r = lax.rem(t, G)
        return (lax.div(t, G), lax.div(r, 2), lax.rem(r, 2), y)

    pair_y = y + 1 - 2 * lax.rem(y, 2)
    weight_pair = (z, x, core, pair_y)
    token_pair = (z, x, core, Y - 1 - y)
    sibling = (z, x, 1 - core, y)

    def rc(src, dst, send, recv, dev):
        return pltpu.make_async_remote_copy(
            src_ref=src, dst_ref=dst, send_sem=send, recv_sem=recv, device_id=dev, device_id_type=MESH
        )

    def drain(ref, sem):
        pltpu.make_async_copy(ref, ref, sem).wait()

    barrier = pltpu.get_barrier_semaphore()

    def greet(dev):
        pl.semaphore_signal(barrier, inc=1, device_id=dev, device_id_type=MESH)

    def tail_copies():
        last = pl.ds(n_pos - 16, 16)
        dev = ep_peer(1)
        return [
            rc(src.at[last, :], dst, s.tail_s.at[k], s.tail_r.at[k], dev)
            for k, (src, dst) in enumerate(
                ((i.heads, s.tail_heads), (i.write, s.tail_write), (i.read, s.tail_read))
            )
        ]

    def weight_copy(k, c):
        src = (i.gate_w, i.up_w, i.down_w)[k].at[0]
        if k < 2:
            src, dst = src.at[COLS[c], :], s.pgu.at[k, COLS[c], :]
        else:
            src, dst = src.at[:, COLS[c]], s.pdown.at[:, COLS[c]]
        return rc(src, dst, s.w_s.at[k // 2], s.w_r.at[k // 2, c], weight_pair)

    shared_full = (s.full_gate, s.full_up, s.full_down)

    def piece(t, slot, q, count=1):
        ref = shared_full[t]
        n = ref.shape[1] // G
        return ref.at[slot, pl.ds(pl.multiple_of(q * n, n), count * n), :]

    def sh_y(t):
        q = core * X + x
        return rc(piece(t, 0, q), piece(t, 1, q), s.shy_s.at[t], s.shy_r.at[t], token_pair)

    def sh_x_start(t, d):
        part = piece(t, 1, core * X + x)
        rc(part, part, s.shx_s.at[t], s.shx_r.at[t], x_peer(d)).start()

    def sh_x_drain(t, sem):
        drain(piece(t, 1, 0, X - 1), sem.at[t])

    def sh_c(t):
        part = piece(t, 1, core * X, X)
        return rc(part, part, s.shc_s.at[t], s.shc_r.at[t], sibling)

    def shared_rows():
        return rc(s.normed, s.pair_normed, s.st_s.at[0], s.st_r.at[0], weight_pair)

    def shared_return():
        return rc(s.sh_send, s.sh_recv, s.st_s.at[1], s.st_r.at[1], weight_pair)

    def sy(c):
        part = (slice(None), slice(None), COLS[c])
        return rc(s.toks.at[0].at[part], s.toks.at[1].at[part], s.y_s.at[0], s.y_r.at[0, c], token_pair)

    def ry(c):
        return rc(s.ysend.at[:, COLS[c]], s.yrecv.at[:, COLS[c]], s.y_s.at[1], s.y_r.at[1, c], token_pair)

    def spread_z(src, dst, c, k):
        @pl.loop(1, Z)
        def _(d):
            rc(
                src.at[lax.rem(z + d, Z), :, COLS[c]], dst.at[z, :, COLS[c]], s.z_s.at[k], s.z_r.at[k, c], z_peer(d)
            ).start()

    def spread_g(src, dst, c, k):
        @pl.loop(1, G)
        def _(d):
            rc(
                src.at[lax.rem(g + d, G), :, COLS[c]], dst.at[g, :, COLS[c]], s.g_s.at[k], s.g_r.at[k, c], g_peer(d)
            ).start()

    def seven(ref, c, sem, k):
        drain(ref.at[pl.ds(0, 7), :, COLS[c]], sem.at[k, c])

    def mix_g(src, dst, k, d):
        rc(src.at[lax.rem(g + d, G)], dst.at[g], s.m_s.at[k], s.m_r.at[k], g_peer(d)).start()

    def mix_drain(ref, sem, k):
        drain(ref.at[pl.ds(0, 7)], sem.at[k])

    bring = []

    def fetched(src, dst):
        bring.append((src, dst))
        return pltpu.make_async_copy(src, dst, s.loc.at[len(bring) - 1])

    small_in = [
        fetched(src, dst)
        for src, dst in (
            (i.routes, s.routes),
            (i.scores, s.scores),
            (i.row_gain, s.row_gain),
            (i.rows, s.rows),
            (i.write, s.write),
            (i.read, s.read),
            (i.step, s.step),
            (i.extra, s.extra),
            (i.decay, s.decay),
            (i.head_taps, s.head_taps),
            (i.write_taps, s.write_taps),
            (i.read_taps, s.read_taps),
            (i.mix_gain, s.mix_gain),
        )
    ]
    local = dict(
        heads=fetched(i.heads, s.heads),
        gates=fetched(i.gates, s.gates),
        perm=fetched(i.perm, s.perm),
        sh_gate=fetched(i.sh_gate, s.full_gate.at[0]),
        sh_up=fetched(i.sh_up, s.full_up.at[0]),
        sh_down=fetched(i.sh_down, s.full_down.at[0]),
        gate=fetched(i.gate_w.at[0], s.ogate),
        up=fetched(i.up_w.at[0], s.oup),
        down=fetched(i.down_w.at[0], s.odown),
        mixw=fetched(i.mix_weight, s.mixw),
    )
    for copy in small_in[:4]:
        copy.start()
    @pl.loop(1, Z)
    def _(d):
        greet(z_peer(d))
        greet(g_peer(d))

    @pl.loop(1, Y)
    def _(d):
        greet(y_peer(d))

    greet(ep_peer(1))
    greet(ep_peer(-1))
    local = Names(local.keys(), local.values())
    small_in[0].wait()
    small_in[1].wait()
    route = s.routes[...]
    score = s.scores[...].astype(f32)
    weight = score / jnp.sum(score, axis=0, keepdims=True) * route_scale
    expert_iota = lax.broadcasted_iota(jnp.int32, (Z * G, tok), 0)
    hot = [(route[k : k + 1, :] == expert_iota).astype(f32) for k in range(2)]
    earlier = (
        lax.broadcasted_iota(jnp.int32, (tok, tok), 0) < lax.broadcasted_iota(jnp.int32, (tok, tok), 1)
    ).astype(bf16)
    before = dot((hot[0] + hot[1]).astype(bf16), earlier)
    slot_iota = lax.broadcasted_iota(jnp.int32, (slots, tok), 0)
    pick = jnp.zeros((slots, tok), f32)
    pick_w = jnp.zeros((slots, tok), f32)
    for k in range(2):
        rank = jnp.sum(before * hot[k], axis=0, keepdims=True).astype(jnp.int32)
        here = slot_iota == route[k : k + 1, :] * CAP + rank
        pick = pick + here.astype(f32)
        pick_w = pick_w + jnp.where(here, weight[k : k + 1, :], 0.0)
    s.pick_w[...] = pick_w
    pick = pick.astype(bf16)
    for copy in small_in[4:] + list(local.__dict__.values()):
        copy.start()
    small_in[2].wait()
    small_in[3].wait()
    rows = s.rows[...].astype(f32)
    normed = (
        rows * lax.rsqrt(jnp.mean(rows * rows, axis=1, keepdims=True) + eps_norm) * s.row_gain[...]
    ).astype(bf16)
    s.normed[...] = normed
    pl.semaphore_wait(barrier, (Z - 1) + (G - 1) + (Y - 1) + 2)

    def select(c):
        part = dot(pick, s.normed[:, COLS[c]]).astype(bf16)
        s.own[:, :, COLS[c]] = part.reshape(Z, zrows, -1)
        spread_z(s.own, s.recv1, c, 0)

    weight_copy(0, 0).start()
    weight_copy(1, 0).start()
    select(0)
    for copy in tail_copies():
        copy.start()
    for t in range(3):
        (local.sh_gate, local.sh_up, local.sh_down)[t].wait()
        sh_y(t).start()
    for c in range(1, CHUNKS):
        weight_copy(0, c).start()
        weight_copy(1, c).start()
        select(c)
    for c in range(CHUNKS):
        weight_copy(2, c).start()
    shared_rows().start()
    s.recv1[z] = s.own[z]

    ext = s.ext

    def mixer_conv():
        local.heads.wait()
        for copy in tail_copies():
            copy.wait_recv()
        has_before = (ep > 0).astype(f32)
        for copy in small_in[4:]:
            copy.wait()
        col = 0
        for src, tail in ((s.heads, s.tail_heads), (s.write, s.tail_write), (s.read, s.tail_read)):
            w = src.shape[1]
            ext[0:16, col : col + w] = tail[...].astype(f32) * has_before
            ext[16 : 16 + n_pos, col : col + w] = src[...].astype(f32)
            col += w

        def conv(taps_ref, col):
            w = taps_ref.shape[1]
            taps = taps_ref[...].astype(f32)
            total = jnp.zeros((n_pos, w), f32)
            for j in range(taps.shape[0]):
                total = total + taps[j : j + 1, :] * ext[13 + j : 13 + j + n_pos, col : col + w]
            return silu(total)

        s.hv[...] = conv(s.head_taps, 0)
        s.wv[...] = conv(s.write_taps, chans)
        s.rv[...] = conv(s.read_taps, chans + STATE)

    def row_col():
        return (
            lax.broadcasted_iota(jnp.int32, (n_pos, n_pos), 0),
            lax.broadcasted_iota(jnp.int32, (n_pos, n_pos), 1),
        )

    def mixer_states():
        pre = s.step[...]
        step = jnp.maximum(pre, 0.0) + jnp.log1p(jnp.exp(-jnp.abs(pre)))
        eye = lax.broadcasted_iota(jnp.int32, (heads, heads), 0) == lax.broadcasted_iota(
            jnp.int32, (heads, heads), 1
        )
        decay = jnp.sum(jnp.where(eye, s.decay[...], 0.0), axis=1, keepdims=True)
        rate = -jnp.exp(decay) * step + s.extra[...]
        pos_r, pos_c = row_col()
        cum = dot(rate, (pos_r <= pos_c).astype(f32), highest)
        s.cum[...] = cum
        total_decay = cum[:, n_pos - 1 : n_pos]
        lane = lax.broadcasted_iota(jnp.int32, (heads, chans), 1)
        first = lax.broadcasted_iota(jnp.int32, (heads, chans), 0) * HEAD_DIM
        spread = ((lane >= first) & (lane < first + HEAD_DIM)).astype(f32)
        xw = s.hv[...] * dot_t(step, spread, highest)
        s.hv[...] = xw
        s.cum_x[...] = dot_t(jnp.exp(cum), spread, highest)
        xe = xw * dot_t(jnp.exp(total_decay - cum), spread, highest)
        decay_x = dot_t(jnp.broadcast_to(total_decay, (heads, 8)), spread, highest)
        states = dot_t(s.wv[...], xe, highest)
        for j in range(G):
            s.st_send[j] = states[:, j * per : (j + 1) * per].astype(bf16)
            s.dec_send[j] = decay_x[:, j * per : (j + 1) * per]
        s.st_got[g] = s.st_send[g]
        s.dec_got[g] = s.dec_send[g]
        s.affinity[...] = lax.dot_general(
            s.rv[...], s.wv[...], (((1,), (1,)), ((), ())), preferred_element_type=f32, precision=highest
        )

    def mixer_scan(pairs):
        cum = s.cum[...]
        cum_t = jnp.transpose(cum)
        affinity = s.affinity[...]
        pos_r, pos_c = row_col()
        low = pos_r >= pos_c
        pair_lane = lax.broadcasted_iota(jnp.int32, (n_pos, 2 * HEAD_DIM), 1) < HEAD_DIM
        for p in pairs:
            cols = slice(p * 2 * HEAD_DIM, (p + 1) * 2 * HEAD_DIM)
            xp = s.hv[:, cols]
            both = []
            for h in (2 * p, 2 * p + 1):
                gap = cum_t[:, h : h + 1] - cum[h : h + 1, :]
                within = jnp.exp(jnp.where(low, gap, -jnp.inf))
                both.append(dot(affinity * within, xp, highest))
            s.scan[:, cols] = jnp.where(pair_lane, both[0], both[1])

    def mixer_group():
        mix_drain(s.st_got, s.m_r, 0)
        mix_drain(s.dec_got, s.m_r, 3)
        run = jnp.zeros((STATE, per), f32)
        run_d = jnp.zeros((8, per), f32)
        for j in range(G):
            s.enter[j, 0:STATE, :] = run
            s.enter[j, STATE : STATE + 8, :] = run_d
            d_j = s.dec_got[j]
            run = s.st_got[j].astype(f32) + jnp.exp(d_j[0:1, :]) * run
            run_d = run_d + d_j
        s.tot_send[0:STATE, :] = run
        s.tot_send[STATE : STATE + 8, :] = run_d

        @pl.loop(1, Z)
        def _(d):
            rc(s.tot_send, s.tot_got.at[z], s.m_s.at[1], s.m_r.at[1], z_peer(d)).start()

        s.tot_got[z] = s.tot_send[...]

    def mixer_enter():
        mix_drain(s.tot_got, s.m_r, 1)
        run = jnp.zeros((STATE, per), f32)
        for j in range(Z):
            new = s.tot_got[j, 0:STATE, :] + jnp.exp(s.tot_got[j, STATE : STATE + 1, :]) * run
            run = jnp.where(j < z, new, run)
        for j in range(G):
            entry = s.enter[j, 0:STATE, :] + jnp.exp(s.enter[j, STATE : STATE + 1, :]) * run
            s.in_send[j] = entry.astype(bf16)
        for d in range(1, G):
            mix_g(s.in_send, s.in_got, 2, d)
        s.in_got[g] = s.in_send[g]

    def mixer_finish():
        mix_drain(s.in_got, s.m_r, 2)
        local.gates.wait()
        rv = s.rv[...]
        square = jnp.zeros((n_pos, 1), f32)
        for j in range(G):
            cols = slice(j * per, (j + 1) * per)
            carried = dot(rv, s.in_got[j].astype(f32), highest) * s.cum_x[:, cols]
            gated = (s.scan[:, cols] + carried) * silu(s.gates[:, cols].astype(f32))
            s.scan[:, cols] = gated
            square = square + jnp.sum(gated * gated, axis=1, keepdims=True)
        scale = lax.rsqrt(square / chans + eps_norm)
        mixed = (s.scan[...] * scale * s.mix_gain[...]).astype(bf16)
        local.mixw.wait()
        mb = n_pos // Y
        for c in range(4):
            cols = slice(c * (width // 4), (c + 1) * (width // 4))
            part = dot(mixed, s.mixw[:, cols]).astype(bf16)
            for j in range(Y):
                s.mix_send[j, :, cols] = part[j * mb : (j + 1) * mb, :]
        s.mix_got[y] = s.mix_send[y]

    def mixer_send():
        @pl.loop(1, Y)
        def _(d):
            rc(
                s.mix_send.at[lax.rem(y + d, Y)], s.mix_got.at[y], s.rs_s.at[0], s.rs_r.at[0], y_peer(d)
            ).start()

    def shared_x(t, d):
        if d == 1:
            sh_y(t).wait_recv()
        sh_x_start(t, d)

    def shared_c():
        for t in range(3):
            sh_x_drain(t, s.shx_r)
            sh_c(t).start()

    def shared_hidden(v, slot):
        return (silu(dot(v, s.full_gate[slot])) * dot(v, s.full_up[slot])).astype(bf16)

    def shared_down(h, q):
        cols = slice(q * (width // 4), (q + 1) * (width // 4))
        return cols, dot(h[0], s.full_down[0, :, cols]) + dot(h[1], s.full_down[1, :, cols])

    def shared_own():
        for t in range(3):
            sh_c(t).wait_recv()
        v = s.normed[...]
        h = (shared_hidden(v, 0), shared_hidden(v, 1))
        for q in range(4):
            cols, new = shared_down(h, q)
            s.sh_own[:, cols] = new

    def shared_pair():
        shared_rows().wait_recv()
        v = s.pair_normed[...]
        h = (shared_hidden(v, 0), shared_hidden(v, 1))
        for q in range(4):
            cols, new = shared_down(h, q)
            s.sh_send[:, cols] = new.astype(bf16)
        shared_return().start()

    def stage_a(c):
        seven(s.recv1, c, s.z_r, 0)
        moved = dot(s.perm[...], s.recv1[:, :, COLS[c]].reshape(slots, -1)).astype(bf16)
        s.perm1[:, :, COLS[c]] = moved.reshape(G, Z * CAP, -1)
        spread_g(s.perm1, s.toks.at[0], c, 0)
        s.toks[0, g, :, COLS[c]] = s.perm1[g, :, COLS[c]]

    def gate_up(t, c):
        v = s.toks[t, :, :, COLS[c]].reshape(slots, -1)
        for acc, refs in ((s.accg, (s.ogate, s.pgu.at[0])), (s.accu, (s.oup, s.pgu.at[1]))):
            for n, ref in enumerate(refs):
                cols = slice(n * ff, (n + 1) * ff)
                new = dot(v, ref[COLS[c], :])
                if c > 0:
                    new = new + acc[t, :, cols]
                acc[t, :, cols] = new

    def stage_b(c):
        seven(s.toks.at[0], c, s.g_r, 0)
        sy(c).start()

    def own_rows(c):
        if c == 0:
            local.gate.wait()
            local.up.wait()
        drain(s.pgu.at[:, COLS[c], :], s.w_r.at[0, c])
        gate_up(0, c)

    def pair_rows(c):
        sy(c).wait_recv()
        gate_up(1, c)

    def hide(t):
        s.hidden[t] = (silu(s.accg[t]) * s.accu[t]).astype(bf16)

    def down(t, c):
        return dot(s.hidden[t, :, 0:ff], s.odown[:, COLS[c]]) + dot(s.hidden[t, :, ff : 2 * ff], s.pdown[:, COLS[c]])

    def back_d(c):
        if c >= CHUNKS:
            return
        if c == 0:
            local.down.wait()
        weight_copy(2, c).wait_recv()
        s.ysend[:, COLS[c]] = down(1, c).astype(bf16)
        ry(c).start()

    def back_e(c):
        mine = down(0, c)
        ry(c).wait_recv()
        total = (mine + s.yrecv[:, COLS[c]].astype(f32)).astype(bf16)
        s.back2[:, :, COLS[c]] = total.reshape(G, Z * CAP, -1)
        spread_g(s.back2, s.got2, c, 1)
        s.got2[g, :, COLS[c]] = s.back2[g, :, COLS[c]]

    def back_f(c):
        seven(s.got2, c, s.g_r, 1)
        moved = dot(s.perm[...], s.got2[:, :, COLS[c]].reshape(slots, -1)).astype(bf16)
        s.back1[:, :, COLS[c]] = moved.reshape(Z, zrows, -1)
        spread_z(s.back1, s.got1, c, 1)
        s.got1[z, :, COLS[c]] = s.back1[z, :, COLS[c]]

    def weights_by_row():
        pick_w = jnp.transpose(s.pick_w[...])
        w_hi = pick_w.astype(bf16)
        s.w_hi[...] = w_hi
        s.w_lo[...] = (pick_w - w_hi.astype(f32)).astype(bf16)

    def early_sends():
        for copy in tail_copies():
            copy.wait_send()
        drain(s.pgu, s.w_s.at[0])
        drain(s.pdown, s.w_s.at[1])
        drain(s.toks.at[0], s.y_s.at[0])
        drain(s.own.at[pl.ds(0, Z - 1)], s.z_s.at[0])
        drain(s.perm1.at[pl.ds(0, G - 1)], s.g_s.at[0])
        for t in range(3):
            sh_y(t).wait_send()
            sh_x_drain(t, s.shx_s)
            sh_c(t).wait_send()
        mix_drain(s.st_got, s.m_s, 0)
        mix_drain(s.dec_got, s.m_s, 3)
        mix_drain(s.tot_got, s.m_s, 1)
        mix_drain(s.in_got, s.m_s, 2)

    extras = {
        1: lambda: mixer_states(),
        2: lambda: mixer_scan(range(0, 2)),
        3: lambda: mixer_scan(range(2, 4)),
        4: lambda: mixer_scan(range(4, 6)),
        5: lambda: mixer_scan(range(6, 8)),
    }
    mixer_conv()
    local.perm.wait()
    for c in range(CHUNKS):
        stage_a(c)
        if c >= 1:
            stage_b(c - 1)
        if c in extras:
            extras[c]()
        if 1 <= c < G:
            mix_g(s.st_send, s.st_got, 0, c)
            mix_g(s.dec_send, s.dec_got, 3, c)
        if c >= 4:
            own_rows(c - 4)
        if c >= 5:
            pair_rows(c - 5)
    stage_b(CHUNKS - 1)
    mixer_group()
    for t in range(3):
        for d in range(1, X):
            shared_x(t, d)
    for c in range(CHUNKS - 4, CHUNKS):
        own_rows(c)
        pair_rows(c - 1)
    pair_rows(CHUNKS - 1)
    hide(1)
    back_d(0)
    back_d(1)
    hide(0)
    back_d(2)
    after = {
        0: lambda: mixer_enter(),
        1: lambda: shared_c(),
        2: lambda: mixer_finish(),
        3: lambda: shared_own(),
        4: lambda: weights_by_row(),
        5: lambda: shared_pair(),
        7: lambda: early_sends(),
        CHUNKS: lambda: mixer_send(),
    }
    for c in range(CHUNKS + 1):
        back_d(c + 3)
        if c < CHUNKS:
            back_e(c)
        if c >= 1:
            back_f(c - 1)
        if c in after:
            after[c]()

    def moe_copy(c):
        return pltpu.make_async_copy(s.moe_res.at[:, COLS[c]], moe_out.at[:, COLS[c]], s.out.at[0])

    def mix_sum():
        drain(s.mix_got.at[pl.ds(0, Y - 1)], s.rs_r.at[0])
        mix = jnp.zeros(s.mix_res.shape, f32)
        for j in range(Y):
            mix = mix + s.mix_got[j].astype(f32)
        s.mix_res[...] = mix.astype(bf16)

    mix_copy = pltpu.make_async_copy(s.mix_res, mix_out, s.out.at[1])
    shared_rows().wait_send()
    shared_return().wait()
    drain(s.ysend, s.y_s.at[1])
    for c in range(CHUNKS):
        if c == CHUNKS - 1:
            drain(s.back2.at[pl.ds(0, G - 1)], s.g_s.at[1])
            drain(s.back1.at[pl.ds(0, Z - 1)], s.z_s.at[1])
            mix_sum()
            mix_copy.start()
            drain(s.mix_send.at[pl.ds(0, Y - 1)], s.rs_s.at[0])
        seven(s.got1, c, s.z_r, 1)
        v = s.got1[:, :, COLS[c]].reshape(slots, -1)
        shared = s.sh_own[:, COLS[c]] + s.sh_recv[:, COLS[c]].astype(f32)
        total = dot(s.w_hi[...], v) + dot(s.w_lo[...], v) + shared
        s.moe_res[:, COLS[c]] = total.astype(bf16)
        moe_copy(c).start()
    mix_copy.wait()
    drain(s.moe_res, s.out.at[0])


def settle(mix_in, moe_in, mix_out, moe_out, mix, moe, sems):
    pairs = ((mix_in, mix, mix_out), (moe_in, moe, moe_out))
    into = [pltpu.make_async_copy(a, v, sems.at[k]) for k, (a, v, _) in enumerate(pairs)]
    out = [pltpu.make_async_copy(v, b, sems.at[k + 2]) for k, (_, v, b) in enumerate(pairs)]
    for copy in into:
        copy.start()
    for arrived, copy in zip(into, out):
        arrived.wait()
        copy.start()
    for copy in out:
        copy.wait()


def local(
    heads, write, read, gates, step, extra, decay, head_taps, write_taps, read_taps, mix_gain,
    mix_weight, rows, row_gain, routes, scores, gate_w, up_w, down_w, sh_gate, sh_up, sh_down,
):
    n_pos, chans = heads.shape
    tok, width = rows.shape
    ff = gate_w.shape[2]
    sff = sh_gate.shape[1]
    slots = Z * G * CAP
    per = chans // G
    order = np.arange(slots).reshape(G, Z, CAP).transpose(1, 0, 2).reshape(-1)
    perm = jnp.asarray(np.eye(slots, dtype=np.float32)[order], bf16)
    dma = pltpu.SemaphoreType.DMA
    blocks = (Z, G * CAP, width)
    scratch = dict(
        tail_heads=((16, chans), bf16),
        tail_write=((16, STATE), bf16),
        tail_read=((16, STATE), bf16),
        ogate=((width, ff), bf16),
        oup=((width, ff), bf16),
        odown=((ff, width), bf16),
        pgu=((2, width, ff), bf16),
        pdown=((ff, width), bf16),
        mixw=((chans, width), bf16),
        full_gate=((2, width, sff), bf16),
        full_up=((2, width, sff), bf16),
        full_down=((2, sff, width), bf16),
        pair_normed=((tok, width), bf16),
        sh_send=((tok, width), bf16),
        sh_recv=((tok, width), bf16),
        gates=((n_pos, chans), bf16),
        normed=((tok, width), bf16),
        sh_own=((tok, width), f32),
        pick_w=((slots, tok), f32),
        w_hi=((tok, slots), bf16),
        w_lo=((tok, slots), bf16),
        own=(blocks, bf16),
        recv1=(blocks, bf16),
        perm1=(blocks, bf16),
        toks=((2, *blocks), bf16),
        accg=((2, slots, 2 * ff), f32),
        accu=((2, slots, 2 * ff), f32),
        hidden=((2, slots, 2 * ff), bf16),
        ysend=((slots, width), bf16),
        yrecv=((slots, width), bf16),
        back2=(blocks, bf16),
        got2=(blocks, bf16),
        back1=(blocks, bf16),
        got1=(blocks, bf16),
        ext=((n_pos + 16, chans + 2 * STATE), f32),
        hv=((n_pos, chans), f32),
        wv=((n_pos, STATE), f32),
        rv=((n_pos, STATE), f32),
        cum=((step.shape[0], n_pos), f32),
        affinity=((n_pos, n_pos), f32),
        cum_x=((n_pos, chans), f32),
        scan=((n_pos, chans), f32),
        st_send=((G, STATE, per), bf16),
        st_got=((G, STATE, per), bf16),
        dec_send=((G, 8, per), f32),
        dec_got=((G, 8, per), f32),
        enter=((G, STATE + 8, per), f32),
        tot_send=((STATE + 8, per), f32),
        tot_got=((Z, STATE + 8, per), f32),
        in_send=((G, STATE, per), bf16),
        in_got=((G, STATE, per), bf16),
        mix_send=((Y, n_pos // Y, width), bf16),
        mix_got=((Y, n_pos // Y, width), bf16),
        mix_res=((n_pos // Y, width), bf16),
        moe_res=((tok, width), bf16),
    )
    sems = dict(
        tail_s=(3,), tail_r=(3,), w_s=(2,), w_r=(2, CHUNKS), shy_s=(3,), shy_r=(3,), shx_s=(3,), shx_r=(3,), shc_s=(3,),
        shc_r=(3,), st_s=(2,), st_r=(2,), z_s=(2,), z_r=(2, CHUNKS), g_s=(2,), g_r=(2, CHUNKS), y_s=(2,),
        y_r=(2, CHUNKS), m_s=(4,), m_r=(4,), rs_s=(1,), rs_r=(1,), loc=(23,), out=(2,),
    )
    inputs = dict(
        gates=gates, mix_weight=mix_weight, gate_w=gate_w, up_w=up_w, down_w=down_w, sh_gate=sh_gate, sh_up=sh_up,
        sh_down=sh_down,
    )
    copied = dict(
        heads=heads, write=write, read=read, step=step, extra=extra, decay=decay.reshape(1, -1), head_taps=head_taps,
        write_taps=write_taps, read_taps=read_taps, mix_gain=mix_gain.reshape(1, -1), rows=rows,
        row_gain=row_gain.reshape(1, -1), routes=routes.T, scores=scores.T, perm=perm,
    )
    scratch.update((n, (v.shape, v.dtype)) for n, v in copied.items())
    inputs.update(copied)
    names = list(scratch) + list(sems)
    shapes = [pltpu.VMEM(*v) for v in scratch.values()] + [dma(v) for v in sems.values()]
    hbm = pl.BlockSpec(memory_space=pl.ANY)
    outs = (
        jax.ShapeDtypeStruct((n_pos // Y, width), bf16),
        jax.ShapeDtypeStruct((tok, width), bf16),
    )
    results = pl.pallas_call(
        make_kernel(list(inputs), names),
        name="mixer_moe",
        out_shape=outs,
        in_specs=[hbm] * len(inputs),
        out_specs=(hbm, hbm),
        scratch_shapes=shapes,
        compiler_params=pltpu.CompilerParams(
            collective_id=0, has_side_effects=True, vmem_limit_bytes=67043328
        ),
    )(*inputs.values())
    return pl.pallas_call(
        settle,
        name="settle",
        out_shape=outs,
        in_specs=[hbm] * 2,
        out_specs=(hbm, hbm),
        scratch_shapes=[pltpu.VMEM(v.shape, v.dtype) for v in outs] + [dma((4,))],
    )(*results)


def solution(mesh):
    split = Mesh(mesh.devices.reshape(8, 4, 2, mesh.shape["tp"]), ("ep_0", "ep_1", "ep_2", "tp"))
    placed = (
        P(EP, "tp"),
        P(EP, "tp"),
        P(EP, "tp"),
        P(EP, "tp"),
        P("tp", EP),
        P("tp", EP),
        P("tp"),
        P(None, "tp"),
        P(None, "tp"),
        P(None, "tp"),
        P("tp"),
        P("tp", None),
        P(EP_TP, None),
        P(),
        P(EP_TP, None),
        P(EP_TP, None),
        P(EP, None, "tp"),
        P(EP, None, "tp"),
        P(EP, "tp", None),
        P(None, "tp"),
        P(None, "tp"),
        P("tp", None),
    )
    return jax.shard_map(
        local,
        mesh=split,
        in_specs=placed,
        out_specs=(P(EP_TP, None), P(EP_TP, None)),
        check_vma=False,
    )
```
